32 devices in a mesh: grp: 2 (over y), dp: 2 (over x), kv: 4 (over z), tp: 2 (over core).
Axes of the slice: x: 2, y: 2, z: 4, core: 2. Of those that a mesh axis runs over, the one named last changes fastest.
Arguments:
- tokens: bfloat16 [32, 2048], P(('grp', 'dp'), ('kv', 'tp')), parts along dimension 0, may hold values from -24 to 24
- memory: float32 [32, 12, 16384], P(('grp', 'dp', 'kv', 'tp')), parts along dimension 0, may hold values from -3 to 3
- mix_gain: float32 [2048], replicated, may hold values from 0.1 to 1.9
- w_query: bfloat16 [2048, 1536], P(None, ('kv', 'tp')), may hold values from -0.125 to 0.125
- w_key: bfloat16 [2048, 1536], P(None, ('kv', 'tp')), may hold values from -0.125 to 0.125
- w_value: bfloat16 [2048, 1536], P(None, ('kv', 'tp')), may hold values from -0.125 to 0.125
- w_gate: bfloat16 [2048, 1536], P(None, ('kv', 'tp')), may hold values from -0.125 to 0.125
- w_beta: bfloat16 [2048, 12], replicated, may hold values from -0.125 to 0.125
- w_decay: bfloat16 [2048, 12], replicated, may hold values from -0.125 to 0.125
- decay_rate: float32 [12], replicated, may hold values from 0.1 to 3
- decay_bias: float32 [12], replicated, may hold values from -2 to 1
- head_gain: float32 [128], replicated, may hold values from 0.1 to 1.9
- w_out: bfloat16 [1536, 2048], P(None, ('kv', 'tp')), may hold values from -0.15625 to 0.15625
- ffn_gain: float32 [2048], replicated, may hold values from 0.1 to 1.9
- w_up: bfloat16 [2048, 8192], P(None, ('kv', 'tp')), may hold values from -0.125 to 0.125
- w_down: bfloat16 [8192, 2048], P(('kv', 'tp')), may hold values from -0.09375 to 0.09375
Outputs:
- layer_out: bfloat16 [32, 2048], P(('grp', 'dp'), ('kv', 'tp')), parts along dimension 0
- new_memory: float32 [32, 12, 16384], P(('grp', 'dp', 'kv', 'tp')), parts along dimension 0
The draws below stay inside these ranges and needn't reach their ends.
There are 2 independent parts, one for each index of `grp`. The reference program is written for one: setup_inputs(seed, part) draws one part's arguments, and reference() takes and returns one part's arrays. A program takes and returns all parts, laid end to end along the dimension named above; an argument that names none is the same for every part. Nothing has to cross between parts.
All inputs are finite; a program needn't handle non-finite values.
Results may differ from the reference program's by a relative error of at most 0.02.
Values may be sent and summed in bfloat16 or wider, within the bound.
No kernel may reach another device: no remote copies, remote signals or barrier semaphores. Data moves between devices by JAX's collectives and lax.ppermute only.
A program may use at most 64 MiB of HBM per device.

```python
import math
import jax
import jax.numpy as jnp
from jax import lax

D = 2048
HEADS = 12
HEAD_DIM = 128
FF = 8192
BATCH = 16


def draw_tokens(key, part):
    streams = jax.random.split(key, 3)
    trend = jnp.exp(jnp.linspace(math.log(0.5), math.log(1.5), D)).astype(jnp.float32)
    rough = jnp.exp(jax.random.uniform(streams[0], (D,), jnp.float32, -0.5, 0.5))
    row_scale = jnp.exp(jax.random.uniform(streams[1], (BATCH, 1), jnp.float32, -0.7, 0.7))
    base = jax.random.normal(streams[2], (BATCH, D), jnp.float32)
    values = jnp.clip(base * row_scale * trend * rough, -24.0, 24.0)
    return values.astype(jnp.bfloat16)


def strengthened(drawn, stream_key, source, target, shards_of, factor):
    owner, partner = [(jnp.arange(drawn.shape[axis_at]) // (drawn.shape[axis_at] // shards_of)).reshape([-1 if axis == axis_at else 1 for axis in range(drawn.ndim)]) for axis_at in (source, target)]
    chosen = jax.random.permutation(stream_key, shards_of)[partner]
    strong = (owner == chosen) | (owner == (partner + shards_of // 2) % shards_of)
    return jnp.where(strong, factor * drawn, drawn)


def levels(key, dims, shards, low, largest):
    factor_of = 1.0
    for dim, shards_of in shards:
        steps = jax.random.uniform(jax.random.fold_in(jax.random.fold_in(key, 6), dim), (shards_of,), jnp.float32, low / len(shards), largest / len(shards))
        factor_of = factor_of * jnp.repeat(jnp.exp(steps), dims[dim] // shards_of).reshape((-1,) + (1,) * (len(dims) - 1 - dim))
    return factor_of


def gaussian(key, extent, spread, most, shards=(), kind=jnp.bfloat16):
    level = levels(key, extent, shards, -0.22, 0.18) if shards else 1.0
    values = jax.random.normal(key, extent, jnp.float32) * spread * level
    return jnp.minimum(jnp.maximum(values, -most), most).astype(kind)


def noise_with(rng, extent, scale, limit, cuts, heavy, dtype=jnp.bfloat16):
    drawn = scale * jax.random.normal(rng, extent, jnp.float32)
    if cuts:
        drawn = drawn * levels(rng, extent, cuts, -0.22, 0.18)
    return jnp.clip(strengthened(drawn, jax.random.fold_in(rng, 3), *heavy), -limit, limit).astype(dtype)


def setup_inputs(seed: int = 0, part: int = 0) -> dict:
    streams_of = jax.random.split(jax.random.key(seed), 17)
    own_keys = jax.random.split(jax.random.fold_in(streams_of[16], part), 17)
    return {
        "tokens": draw_tokens(jax.random.fold_in(jax.random.fold_in(streams_of[16], part), 71), part),
        "memory": gaussian(own_keys[1], (BATCH, HEADS, HEAD_DIM * HEAD_DIM), 0.5, 3.0, ((0, 16),), jnp.float32),
        "mix_gain": jnp.clip(1.0 + 0.18 * jax.random.normal(streams_of[2], (D,), jnp.float32), 0.1, 1.9),
        "w_query": gaussian(streams_of[3], (D, HEADS * HEAD_DIM), D ** -0.5, 0.125, ((1, 8),)),
        "w_key": gaussian(streams_of[4], (D, HEADS * HEAD_DIM), D ** -0.5, 0.125, ((1, 8),)),
        "w_value": gaussian(streams_of[5], (D, HEADS * HEAD_DIM), D ** -0.5, 0.125, ((1, 8),)),
        "w_gate": gaussian(streams_of[6], (D, HEADS * HEAD_DIM), D ** -0.5, 0.125, ((1, 8),)),
        "w_beta": gaussian(streams_of[7], (D, HEADS), D ** -0.5, 0.125),
        "w_decay": gaussian(streams_of[8], (D, HEADS), D ** -0.5, 0.125),
        "decay_rate": jnp.clip(jnp.exp(jax.random.uniform(streams_of[9], (HEADS,), jnp.float32, math.log(0.1), math.log(3.0))), 0.1, 3.0),
        "decay_bias": jnp.clip(jax.random.uniform(streams_of[10], (HEADS,), jnp.float32, -2.0, 1.0), -2.0, 1.0),
        "head_gain": jnp.clip(1.0 + 0.18 * jax.random.normal(streams_of[11], (HEAD_DIM,), jnp.float32), 0.1, 1.9),
        "w_out": gaussian(streams_of[12], (HEADS * HEAD_DIM, D), (HEADS * HEAD_DIM) ** -0.5, 0.15625, ((1, 8),)),
        "ffn_gain": jnp.clip(1.0 + 0.18 * jax.random.normal(streams_of[13], (D,), jnp.float32), 0.1, 1.9),
        "w_up": gaussian(streams_of[14], (D, FF), D ** -0.5, 0.125, ((1, 8),)),
        "w_down": noise_with(streams_of[15], (FF, D), FF ** -0.5, 0.09375, ((0, 8),), (0, 1, 8, 2.0)),
    }


epsilon = 1e-06

def delta_step(queries, keys_in, values, gates, strength, log_decay, memory, head_gain):
    count = queries.shape[0]
    heads = strength.shape[1]
    size = head_gain.shape[0]
    highest = lax.Precision.HIGHEST
    query_wide = queries.astype(jnp.float32).reshape(count, heads, size)
    key_wide = keys_in.astype(jnp.float32).reshape(count, heads, size)
    value_wide = values.astype(jnp.float32).reshape(count, heads, size)
    gate_wide = gates.astype(jnp.float32).reshape(count, heads, size)
    unit_key = key_wide * lax.rsqrt(lax.optimization_barrier(jnp.sum(key_wide * key_wide, axis=-1, keepdims=True)) + epsilon)
    matrix = memory.reshape(count, heads, size, size)
    recall = jnp.einsum('bhk,bhkv->bhv', unit_key, matrix, precision=highest)
    retain = jnp.exp(log_decay)[:, :, None, None]
    scaled = strength[:, :, None]
    erased = matrix - jnp.einsum('bhk,bhv->bhkv', unit_key, scaled * recall, precision=highest)
    written = jnp.einsum('bhk,bhv->bhkv', unit_key, scaled * value_wide, precision=highest)
    updated = retain * erased + written
    readout = jnp.einsum('bhk,bhkv->bhv', query_wide, updated, precision=highest)
    normed = readout * lax.rsqrt(lax.optimization_barrier(jnp.mean(readout * readout, axis=-1, keepdims=True)) + epsilon)
    normed = normed * head_gain * jax.nn.silu(gate_wide)
    return (updated.reshape(count, heads, size * size), normed.reshape(count, heads * size).astype(jnp.bfloat16))

def reference(tokens, memory, mix_gain, w_query, w_key, w_value, w_gate, w_beta, w_decay, decay_rate, decay_bias, head_gain, w_out, ffn_gain, w_up, w_down):
    width = tokens.shape[1]
    wide = tokens.astype(jnp.float32)
    scale_in = lax.rsqrt(lax.optimization_barrier(jnp.sum(wide * wide, axis=1)) / width + epsilon)[:, None]
    lifted_in = (wide * mix_gain).astype(jnp.bfloat16)

    def project(weight):
        return jnp.dot(lifted_in, weight, preferred_element_type=jnp.float32) * scale_in
    queries = project(w_query).astype(jnp.bfloat16)
    keys_in = project(w_key).astype(jnp.bfloat16)
    values = project(w_value).astype(jnp.bfloat16)
    gates = project(w_gate).astype(jnp.bfloat16)
    strength = jax.nn.sigmoid(project(w_beta))
    log_decay = -decay_rate * jax.nn.softplus(project(w_decay) + decay_bias)
    updated, mixed = delta_step(queries, keys_in, values, gates, strength, log_decay, memory, head_gain)
    branch = jnp.dot(mixed, w_out, preferred_element_type=jnp.float32)
    middle = (wide + branch).astype(jnp.bfloat16)
    middle_wide = middle.astype(jnp.float32)
    scale_mid = lax.rsqrt(lax.optimization_barrier(jnp.sum(middle_wide * middle_wide, axis=1)) / width + epsilon)[:, None]
    lifted_mid = (middle_wide * ffn_gain).astype(jnp.bfloat16)
    hidden = jnp.square(jax.nn.relu(jnp.dot(lifted_mid, w_up, preferred_element_type=jnp.float32) * scale_mid))
    hidden = hidden.astype(jnp.bfloat16)
    layer_out = (middle_wide + jnp.dot(hidden, w_down, preferred_element_type=jnp.float32)).astype(jnp.bfloat16)
    return (layer_out, updated)
```

```python
import jax
import jax.numpy as jnp
from jax import lax
from jax.sharding import PartitionSpec as P


epsilon = 1e-06
axes = ("kv", "tp")


def by_distance(stack, chip):
    count = stack.shape[0]
    rest = stack.shape[1:]
    bit = 1
    while bit < count:
        split = stack.reshape((count // (2 * bit), 2, bit) + rest)
        flipped = jnp.where((chip & bit) != 0, split[:, ::-1], split)
        stack = flipped.reshape((count,) + rest)
        bit *= 2
    return stack


def far(pieces, chips):
    got = [pieces[0]]
    for d in range(1, chips):
        pairs = [(i, i ^ (2 * d + 1)) for i in range(2 * chips)]
        got.append(lax.ppermute(pieces[d], axes, pairs))
    return got


def near(value):
    return lax.ppermute(value, "tp", [(0, 1), (1, 0)])


def merge(mine, other, chip, core):
    count = mine.shape[0]
    own = (jnp.arange(count) == 0).reshape((count,) + (1,) * (mine.ndim - 1))
    low_is_mine = own == (core == 0)
    low = jnp.where(low_is_mine, mine, other)
    high = jnp.where(low_is_mine, other, mine)
    both = by_distance(jnp.stack([low, high], axis=1), chip)
    return both.reshape((2 * count,) + mine.shape[1:])


def gather(piece, chips, chip, core):
    mine = jnp.stack(far([piece] * chips, chips))
    return merge(mine, near(mine), chip, core)


def gather_features(piece, chips, chip, core):
    parts = gather(piece, chips, chip, core)
    return jnp.concatenate([parts[i] for i in range(2 * chips)], axis=1)


def delta_step(queries, keys_in, values, gates, strength, log_decay, memory, head_gain):
    count = queries.shape[0]
    heads = strength.shape[1]
    size = head_gain.shape[0]
    highest = lax.Precision.HIGHEST
    query_wide = queries.astype(jnp.float32).reshape(count, heads, size)
    key_wide = keys_in.astype(jnp.float32).reshape(count, heads, size)
    value_wide = values.astype(jnp.float32).reshape(count, heads, size)
    gate_wide = gates.astype(jnp.float32).reshape(count, heads, size)
    unit_key = key_wide * lax.rsqrt(jnp.sum(key_wide * key_wide, axis=-1, keepdims=True) + epsilon)
    matrix = memory.reshape(count, heads, size, size)
    recall = jnp.einsum("bhk,bhkv->bhv", unit_key, matrix, precision=highest)
    retain = jnp.exp(log_decay)[:, :, None, None]
    scaled = strength[:, :, None]
    erased = matrix - jnp.einsum("bhk,bhv->bhkv", unit_key, scaled * recall, precision=highest)
    written = jnp.einsum("bhk,bhv->bhkv", unit_key, scaled * value_wide, precision=highest)
    updated = retain * erased + written
    readout = jnp.einsum("bhk,bhkv->bhv", query_wide, updated, precision=highest)
    normed = readout * lax.rsqrt(jnp.mean(readout * readout, axis=-1, keepdims=True) + epsilon)
    normed = normed * head_gain * jax.nn.silu(gate_wide)
    return (
        updated.reshape(count, heads, size * size),
        normed.reshape(count, heads * size).astype(jnp.bfloat16),
    )


def per_device(
    chips,
    tokens,
    memory,
    mix_gain,
    w_query,
    w_key,
    w_value,
    w_gate,
    w_beta,
    w_decay,
    decay_rate,
    decay_bias,
    head_gain,
    w_out,
    ffn_gain,
    w_up,
    w_down,
):
    rows = tokens.shape[0]
    owned = memory.shape[0]
    width = mix_gain.shape[0]
    chip = lax.axis_index("kv")
    core = lax.axis_index("tp")
    own_start = lax.axis_index(axes) * owned
    wide = tokens.astype(jnp.float32)

    def lifted_of(whole, gain):
        whole_wide = whole.astype(jnp.float32)
        scale = lax.rsqrt(jnp.sum(whole_wide * whole_wide, axis=1) / width + epsilon)
        return (whole_wide * gain).astype(jnp.bfloat16), scale[:, None]

    def project(value, weight):
        return jnp.dot(value, weight, preferred_element_type=jnp.float32)

    lifted_in, scale_in = lifted_of(gather_features(tokens, chips, chip, core), mix_gain)
    sent = jnp.stack(
        [
            (project(lifted_in, weight) * scale_in).astype(jnp.bfloat16)
            for weight in (w_query, w_key, w_value, w_gate)
        ],
        axis=1,
    )
    strength_all = jax.nn.sigmoid(project(lifted_in, w_beta) * scale_in)
    decay_all = -decay_rate * jax.nn.softplus(project(lifted_in, w_decay) * scale_in + decay_bias)
    strength = lax.dynamic_slice_in_dim(strength_all, own_start, owned, 0)
    log_decay = lax.dynamic_slice_in_dim(decay_all, own_start, owned, 0)

    part = sent.shape[2]
    leaving = by_distance(sent.reshape(chips, 2, owned, 4, part), chip)
    mine = jnp.stack(far([leaving[d] for d in range(chips)], chips))
    other = near(mine)
    pick = lambda both: jnp.where(core == 0, both[:, 0], both[:, 1])
    whole = merge(pick(mine), pick(other), chip, core)
    whole = jnp.transpose(whole, (2, 1, 0, 3)).reshape(4, owned, 2 * chips * part)
    updated, mixed = delta_step(
        whole[0], whole[1], whole[2], whole[3], strength, log_decay, memory, head_gain
    )

    mixed_all = gather(mixed, chips, chip, core).reshape(rows, mixed.shape[1])
    middle = (wide + project(mixed_all, w_out)).astype(jnp.bfloat16)
    middle_wide = middle.astype(jnp.float32)
    lifted_mid, scale_mid = lifted_of(gather_features(middle, chips, chip, core), ffn_gain)
    raised = project(lifted_mid, w_up)
    hidden = jnp.square(jax.nn.relu(raised * scale_mid)).astype(jnp.bfloat16)
    terms = project(hidden, w_down).astype(jnp.bfloat16)

    features = tokens.shape[1]
    blocks = jnp.stack([terms[:, i * 2 * features : (i + 1) * 2 * features] for i in range(chips)])
    leaving = by_distance(blocks, chip)
    total = sum(
        (got.astype(jnp.float32) for got in far([leaving[d] for d in range(chips)], chips))
    )
    low, high = total[:, :features], total[:, features:]
    arrived = near(jnp.where(core == 0, high, low))
    down = jnp.where(core == 0, low, high) + arrived
    layer_out = (middle_wide + down).astype(jnp.bfloat16)
    return (layer_out, updated)


def solution(mesh):
    chips = mesh.shape["kv"]
    placed = (
        P(("grp", "dp"), ("kv", "tp")),
        P(("grp", "dp", "kv", "tp"), None, None),
        P(),
        P(None, ("kv", "tp")),
        P(None, ("kv", "tp")),
        P(None, ("kv", "tp")),
        P(None, ("kv", "tp")),
        P(),
        P(),
        P(),
        P(),
        P(),
        P(None, ("kv", "tp")),
        P(),
        P(None, ("kv", "tp")),
        P(("kv", "tp"), None),
    )

    def step(*arrays):
        return per_device(chips, *arrays)

    return jax.shard_map(
        step,
        mesh=mesh,
        in_specs=placed,
        out_specs=(P(("grp", "dp"), ("kv", "tp")), P(("grp", "dp", "kv", "tp"), None, None)),
        check_vma=False,
    )
```

```python
import functools

import jax
import jax.numpy as jnp
from jax import lax
from jax.experimental import pallas as pl
from jax.experimental.pallas import tpu as pltpu
from jax.sharding import PartitionSpec as P


epsilon = 1e-06
axes = ("kv", "tp")


def by_distance(stack, chip):
    count = stack.shape[0]
    rest = stack.shape[1:]
    bit = 1
    while bit < count:
        split = stack.reshape((count // (2 * bit), 2, bit) + rest)
        flipped = jnp.where((chip & bit) != 0, split[:, ::-1], split)
        stack = flipped.reshape((count,) + rest)
        bit *= 2
    return stack


def far(pieces, chips):
    got = [pieces[0]]
    for d in range(1, chips):
        pairs = [(i, i ^ (2 * d + 1)) for i in range(2 * chips)]
        got.append(lax.ppermute(pieces[d], axes, pairs))
    return got


def near(value):
    return lax.ppermute(value, "tp", [(0, 1), (1, 0)])


def merge(mine, other, chip, core):
    count = mine.shape[0]
    own = (jnp.arange(count) == 0).reshape((count,) + (1,) * (mine.ndim - 1))
    low_is_mine = own == (core == 0)
    low = jnp.where(low_is_mine, mine, other)
    high = jnp.where(low_is_mine, other, mine)
    both = by_distance(jnp.stack([low, high], axis=1), chip)
    return both.reshape((2 * count,) + mine.shape[1:])


def gather(piece, chips, chip, core):
    mine = jnp.stack(far([piece] * chips, chips))
    return merge(mine, near(mine), chip, core)


def gather_features(piece, chips, chip, core):
    parts = gather(piece, chips, chip, core)
    return jnp.concatenate([parts[i] for i in range(2 * chips)], axis=1)


def delta_step(queries, keys_in, values, gates, strength, log_decay, memory, head_gain):
    count = queries.shape[0]
    heads = strength.shape[1]
    size = head_gain.shape[0]
    highest = lax.Precision.HIGHEST
    query_wide = queries.astype(jnp.float32).reshape(count, heads, size)
    key_wide = keys_in.astype(jnp.float32).reshape(count, heads, size)
    value_wide = values.astype(jnp.float32).reshape(count, heads, size)
    gate_wide = gates.astype(jnp.float32).reshape(count, heads, size)
    unit_key = key_wide * lax.rsqrt(jnp.sum(key_wide * key_wide, axis=-1, keepdims=True) + epsilon)
    matrix = memory.reshape(count, heads, size, size)
    recall = jnp.einsum("bhk,bhkv->bhv", unit_key, matrix, precision=highest)
    retain = jnp.exp(log_decay)[:, :, None, None]
    scaled = strength[:, :, None]
    erased = matrix - jnp.einsum("bhk,bhv->bhkv", unit_key, scaled * recall, precision=highest)
    written = jnp.einsum("bhk,bhv->bhkv", unit_key, scaled * value_wide, precision=highest)
    updated = retain * erased + written
    readout = jnp.einsum("bhk,bhkv->bhv", query_wide, updated, precision=highest)
    normed = readout * lax.rsqrt(jnp.mean(readout * readout, axis=-1, keepdims=True) + epsilon)
    normed = normed * head_gain * jax.nn.silu(gate_wide)
    return (
        updated.reshape(count, heads, size * size),
        normed.reshape(count, heads * size).astype(jnp.bfloat16),
    )


def plain_device(
    chips,
    tokens,
    memory,
    mix_gain,
    w_query,
    w_key,
    w_value,
    w_gate,
    w_beta,
    w_decay,
    decay_rate,
    decay_bias,
    head_gain,
    w_out,
    ffn_gain,
    w_up,
    w_down,
):
    rows = tokens.shape[0]
    owned = memory.shape[0]
    width = mix_gain.shape[0]
    chip = lax.axis_index("kv")
    core = lax.axis_index("tp")
    own_start = lax.axis_index(axes) * owned
    wide = tokens.astype(jnp.float32)

    def lifted_of(whole, gain):
        whole_wide = whole.astype(jnp.float32)
        scale = lax.rsqrt(jnp.sum(whole_wide * whole_wide, axis=1) / width + epsilon)
        return (whole_wide * gain).astype(jnp.bfloat16), scale[:, None]

    def project(value, weight):
        return jnp.dot(value, weight, preferred_element_type=jnp.float32)

    lifted_in, scale_in = lifted_of(gather_features(tokens, chips, chip, core), mix_gain)
    sent = jnp.stack(
        [
            (project(lifted_in, weight) * scale_in).astype(jnp.bfloat16)
            for weight in (w_query, w_key, w_value, w_gate)
        ],
        axis=1,
    )
    strength_all = jax.nn.sigmoid(project(lifted_in, w_beta) * scale_in)
    decay_all = -decay_rate * jax.nn.softplus(project(lifted_in, w_decay) * scale_in + decay_bias)
    strength = lax.dynamic_slice_in_dim(strength_all, own_start, owned, 0)
    log_decay = lax.dynamic_slice_in_dim(decay_all, own_start, owned, 0)

    part = sent.shape[2]
    leaving = by_distance(sent.reshape(chips, 2, owned, 4, part), chip)
    mine = jnp.stack(far([leaving[d] for d in range(chips)], chips))
    other = near(mine)
    pick = lambda both: jnp.where(core == 0, both[:, 0], both[:, 1])
    whole = merge(pick(mine), pick(other), chip, core)
    whole = jnp.transpose(whole, (2, 1, 0, 3)).reshape(4, owned, 2 * chips * part)
    updated, mixed = delta_step(
        whole[0], whole[1], whole[2], whole[3], strength, log_decay, memory, head_gain
    )

    mixed_all = gather(mixed, chips, chip, core).reshape(rows, mixed.shape[1])
    middle = (wide + project(mixed_all, w_out)).astype(jnp.bfloat16)
    middle_wide = middle.astype(jnp.float32)
    lifted_mid, scale_mid = lifted_of(gather_features(middle, chips, chip, core), ffn_gain)
    raised = project(lifted_mid, w_up)
    hidden = jnp.square(jax.nn.relu(raised * scale_mid)).astype(jnp.bfloat16)
    terms = project(hidden, w_down).astype(jnp.bfloat16)

    features = tokens.shape[1]
    blocks = jnp.stack([terms[:, i * 2 * features : (i + 1) * 2 * features] for i in range(chips)])
    leaving = by_distance(blocks, chip)
    total = sum(
        (got.astype(jnp.float32) for got in far([leaving[d] for d in range(chips)], chips))
    )
    low, high = total[:, :features], total[:, features:]
    arrived = near(jnp.where(core == 0, high, low))
    down = jnp.where(core == 0, low, high) + arrived
    layer_out = (middle_wide + down).astype(jnp.bfloat16)
    return (layer_out, updated)


def place():
    return lax.axis_index("kv"), lax.axis_index("tp")


def mine_lane(d):
    chip, core = place()
    return 2 * (chip ^ d) + (core if d == 0 else 1 - core)


def other_lane(d):
    chip, core = place()
    return 2 * (chip ^ d) + (1 - core if d == 0 else core)


def span(lane, size):
    return pl.ds(pl.multiple_of(lane * size, size), size)


def dot_rows(left, right):
    return lax.dot_general(left, right, (((1,), (1,)), ((), ())), preferred_element_type=jnp.float32)


def dot(left, right):
    return jnp.dot(left, right, preferred_element_type=jnp.float32)


def call(body, outs, args, scratch=(), work=1e9):
    vmem = pl.BlockSpec(memory_space=pltpu.VMEM)
    return pl.pallas_call(
        body,
        out_shape=[jax.ShapeDtypeStruct(shape, kind) for shape, kind in outs],
        in_specs=[vmem] * len(args),
        out_specs=[vmem] * len(outs),
        scratch_shapes=list(scratch),
        compiler_params=pltpu.CompilerParams(vmem_limit_bytes=16 << 20),
        cost_estimate=pl.CostEstimate(flops=int(work), bytes_accessed=0, transcendentals=0),
    )(*args)


def keep_near(tokens, near_ref):
    near_ref[...] = tokens[...]


def project_piece(piece, lane, gain, weights, lifted, parts):
    size = piece.shape[1]
    wide = piece.astype(jnp.float32)
    ready = (wide * gain[:, span(lane, size)]).astype(jnp.bfloat16)
    lifted[:, span(lane, size)] = ready
    stacked = jnp.concatenate([weight[:, span(lane, size)] for weight in weights], axis=0)
    parts.append((dot_rows(ready, stacked), jnp.sum(wide * wide, axis=1, keepdims=True)))


def project_first(chips, tokens, partner, *refs):
    got, (gain, *rest) = refs[: chips - 1], refs[chips - 1 :]
    weights, (total, squares, lifted) = rest[:4], rest[4:]
    lifted[...] = jnp.zeros_like(lifted)
    parts = []
    project_piece(tokens[...], mine_lane(0), gain, weights, lifted, parts)
    project_piece(partner[...], other_lane(0), gain, weights, lifted, parts)
    for d in range(1, chips):
        project_piece(got[d - 1][...], mine_lane(d), gain, weights, lifted, parts)
    total[...] = sum(part[0] for part in parts)
    squares[...] = jnp.broadcast_to(sum(part[1] for part in parts), squares.shape)


def project_rest(chips, others, before, before_squares, before_lifted, gain, *rest):
    weights, (scale_ref, lifted, *leaving), sent = rest[:4], rest[4:-1], rest[-1]
    lifted[...] = before_lifted[...]
    parts = [(before[...], before_squares[:, :1])]
    for d in range(1, chips):
        project_piece(others[d - 1], other_lane(d), gain, weights, lifted, parts)
    squares = sum(part[1] for part in parts)
    scale = lax.rsqrt(squares / lifted.shape[1] + epsilon)
    total = sum(part[0] for part in parts) * scale
    sent[...] = total.astype(jnp.bfloat16).astype(jnp.float32)
    scale_ref[...] = jnp.broadcast_to(scale, scale_ref.shape)
    chip, _ = place()
    for d in range(chips):
        for c in range(2):
            leaving[d][c : c + 1, :] = sent[pl.ds(2 * (chip ^ d) + c, 1), :]


def column(row, heads):
    there = lax.broadcasted_iota(jnp.int32, (heads, heads), 0)
    here = lax.broadcasted_iota(jnp.int32, (heads, heads), 1)
    return jnp.sum(jnp.where(there == here, row, 0.0), axis=1, keepdims=True)


def own_gates(lifted, scale, w_beta, w_decay, rate, bias, strength, retain):
    heads = w_beta.shape[0]
    lane = mine_lane(0)
    scale_own = scale[pl.ds(lane, 1), :][:, :1]

    def own(weight):
        every = dot_rows(weight[...], lifted[...])
        here = lax.broadcasted_iota(jnp.int32, every.shape, 1) == lane
        return jnp.sum(jnp.where(here, every, 0.0), axis=1, keepdims=True) * scale_own

    value = own(w_decay) + column(bias[...], heads)
    soft = jnp.maximum(value, 0.0) + jnp.log1p(jnp.exp(-jnp.abs(value)))
    decay = jnp.exp(-column(rate[...], heads) * soft)
    beta = 1.0 / (1.0 + jnp.exp(-own(w_beta)))
    strength[...] = jnp.broadcast_to(beta, strength.shape)
    retain[...] = jnp.broadcast_to(decay, retain.shape)


def read_memory(chips, *refs):
    mine, other, strength, retain, memory, head_gain, mixed, unit_ref, write_ref, parts = refs
    heads, size = strength.shape
    chip, core = place()
    part = mine.shape[2] // 4
    across = 2 * part // size
    for there in range(chips):
        d = chip ^ there
        own = mine[d, pl.ds(core, 1), :]
        partner = other[d, pl.ds(core, 1), :]
        straight = (d == 0) == (core == 0)
        low = jnp.where(straight, own, partner)
        high = jnp.where(straight, partner, own)
        for t in range(4):
            cut = slice(t * part, (t + 1) * part)
            pair = jnp.concatenate([low[:, cut], high[:, cut]], axis=1)
            for i in range(across):
                h = there * across + i
                parts[t, h : h + 1, :] = pair[:, i * size : (i + 1) * size]
    query, key, value, gate = parts[0], parts[1], parts[2], parts[3]
    unit = key * lax.rsqrt(jnp.sum(key * key, axis=1, keepdims=True) + epsilon)
    padded = -(-heads // 8) * 8
    pad = [jnp.zeros((padded - heads, size), jnp.float32)] if padded > heads else []
    rest = jnp.zeros((size - 2 * padded, size), jnp.float32)
    turned = jnp.concatenate([unit, *pad, query, *pad, rest], axis=0).T
    recalls, reads = [], []
    for h in range(heads):
        matrix = memory[h]
        recalls.append(jnp.sum(matrix * turned[:, h : h + 1], axis=0, keepdims=True))
        at = padded + h
        reads.append(jnp.sum(matrix * turned[:, at : at + 1], axis=0, keepdims=True))
    recall = jnp.concatenate(recalls, axis=0)
    read = jnp.concatenate(reads, axis=0)
    write = strength[...] * (value - retain[...] * recall)
    readout = retain[...] * read + jnp.sum(unit * query, axis=1, keepdims=True) * write
    normed = readout * lax.rsqrt(jnp.mean(readout * readout, axis=1, keepdims=True) + epsilon)
    normed = normed * head_gain[...] * (gate / (1.0 + jnp.exp(-gate)))
    normed = normed.astype(jnp.bfloat16).astype(jnp.float32)
    for h in range(heads):
        mixed[:, h * size : (h + 1) * size] = normed[h : h + 1]
    unit_ref[...] = unit
    write_ref[...] = write


def mix_out(chips, tokens, own, *refs):
    got, (others, weight, middle, rows) = refs[: chips - 1], refs[chips - 1 :]
    rows[pl.ds(mine_lane(0), 1), :] = own[...]
    rows[pl.ds(other_lane(0), 1), :] = others[0:1]
    for d in range(1, chips):
        rows[pl.ds(mine_lane(d), 1), :] = got[d - 1][...]
        rows[pl.ds(other_lane(d), 1), :] = others[d : d + 1]
    branch = dot(rows[...].astype(jnp.bfloat16), weight[...])
    middle[...] = (tokens[...].astype(jnp.float32) + branch).astype(jnp.bfloat16)


def up_piece(piece, lane, gain, weight, parts):
    size = piece.shape[1]
    wide = piece.astype(jnp.float32)
    ready = (wide * gain[:, span(lane, size)]).astype(jnp.bfloat16)
    parts.append((dot(ready, weight[span(lane, size), :]), jnp.sum(wide * wide, axis=1, keepdims=True)))


def up_first(chips, own, *refs):
    got, (gain, weight, total, squares) = refs[: chips - 1], refs[chips - 1 :]
    parts = []
    for d in range(chips):
        up_piece((got[d - 1] if d else own)[...], mine_lane(d), gain, weight, parts)
    total[...] = sum(part[0] for part in parts)
    squares[...] = jnp.broadcast_to(sum(part[1] for part in parts), squares.shape)


def up_rest(chips, others, before, before_squares, gain, weight, down, hidden_ref, leaving):
    parts = [(before[...], before_squares[:, :1])]
    for d in range(chips):
        up_piece(others[d], other_lane(d), gain, weight, parts)
    scale = lax.rsqrt(sum(part[1] for part in parts) / gain.shape[1] + epsilon)
    raised = jnp.maximum(sum(part[0] for part in parts) * scale, 0.0)
    hidden = (raised * raised).astype(jnp.bfloat16)
    hidden_ref[...] = hidden
    size = leaving.shape[2]
    for d in range(chips):
        leaving[d] = dot(hidden, down[:, span(other_lane(d), size)]).astype(jnp.bfloat16)


def down_own(chips, hidden, down, staying):
    size = staying.shape[2]
    for d in range(chips):
        staying[d] = dot(hidden[...], down[:, span(mine_lane(d), size)])


def kernel_device(
    chips,
    tokens,
    memory,
    mix_gain,
    w_query,
    w_key,
    w_value,
    w_gate,
    w_beta,
    w_decay,
    decay_rate,
    decay_bias,
    head_gain,
    w_out,
    ffn_gain,
    w_up,
    w_down,
):
    f32, bf16 = jnp.float32, jnp.bfloat16
    rows, features = tokens.shape
    width = mix_gain.shape[0]
    heads = w_beta.shape[1]
    size = head_gain.shape[0]
    units = w_up.shape[1]
    part = w_query.shape[1]

    got = far([tokens] * chips, chips)[1:]
    partner = near(tokens)
    (tokens,) = call(keep_near, [(tokens.shape, bf16)], [tokens], work=8e9)
    others = near(jnp.stack(got))
    weights = [weight.T for weight in (w_query, w_key, w_value, w_gate)]
    gain_in = mix_gain.reshape(1, width)
    total, squares, lifted = call(
        functools.partial(project_first, chips),
        [((rows, 4 * part), f32), ((rows, 128), f32), ((rows, width), bf16)],
        [tokens, partner, *got, gain_in, *weights],
    )
    scale_in, lifted, *leaving = call(
        functools.partial(project_rest, chips),
        [((rows, 128), f32), ((rows, width), bf16)] + [((2, 4 * part), f32)] * chips,
        [others, total, squares, lifted, gain_in, *weights],
        [pltpu.VMEM((rows, 4 * part), f32)],
    )
    strength, retain = call(
        own_gates,
        [((heads, size), f32)] * 2,
        [lifted, scale_in, w_beta.T, w_decay.T]
        + [value.reshape(1, heads) for value in (decay_rate, decay_bias)],
    )
    mine = jnp.stack(far(leaving, chips))
    matrix = memory.reshape(heads, size, size)
    mixed, unit, write = call(
        functools.partial(read_memory, chips),
        [((1, heads * size), f32), ((heads, size), f32), ((heads, size), f32)],
        [mine, near(mine), strength, retain, matrix, head_gain.reshape(1, size)],
        [pltpu.VMEM((4, heads, size), f32)],
    )
    updated = retain[:, :1, None] * matrix + unit[:, :, None] * write[:, None, :]

    got = far([mixed] * chips, chips)[1:]
    others = near(jnp.concatenate([mixed] + got, axis=0))
    (middle,) = call(
        functools.partial(mix_out, chips),
        [((rows, features), bf16)],
        [tokens, mixed, *got, others, w_out],
        [pltpu.VMEM((rows, heads * size), f32)],
    )

    got = far([middle] * chips, chips)[1:]
    others = near(jnp.stack([middle] + got))
    gain_mid = ffn_gain.reshape(1, width)
    total, squares = call(
        functools.partial(up_first, chips),
        [((rows, units), f32), ((rows, 128), f32)],
        [middle, *got, gain_mid, w_up],
    )
    hidden, leaving = call(
        functools.partial(up_rest, chips),
        [((rows, units), bf16), ((chips, rows, features), bf16)],
        [others, total, squares, gain_mid, w_up, w_down],
    )
    arrived = near(leaving)
    (staying,) = call(
        functools.partial(down_own, chips), [((chips, rows, features), f32)], [hidden, w_down]
    )
    sums = staying + arrived.astype(f32)
    terms = far([sums[0]] + [sums[d].astype(bf16) for d in range(1, chips)], chips)
    down = sum(term.astype(f32) for term in terms)
    layer_out = (middle.astype(f32) + down).astype(bf16)
    return (layer_out, updated.reshape(memory.shape))


def per_device(chips, *arrays):
    tokens, memory, head_gain = arrays[0], arrays[1], arrays[11]
    fits = (
        memory.shape[0] == 1
        and tokens.shape[0] == 2 * chips
        and tokens.shape[1] % 128 == 0
        and arrays[3].shape[1] % 16 == 0
        and 2 * arrays[3].shape[1] % head_gain.shape[0] == 0
        and head_gain.shape[0] == 128
        and memory.shape[1] <= 32
    )
    return (kernel_device if fits else plain_device)(chips, *arrays)


def solution(mesh):
    chips = mesh.shape["kv"]
    placed = (
        P(("grp", "dp"), ("kv", "tp")),
        P(("grp", "dp", "kv", "tp"), None, None),
        P(),
        P(None, ("kv", "tp")),
        P(None, ("kv", "tp")),
        P(None, ("kv", "tp")),
        P(None, ("kv", "tp")),
        P(),
        P(),
        P(),
        P(),
        P(),
        P(None, ("kv", "tp")),
        P(),
        P(None, ("kv", "tp")),
        P(("kv", "tp"), None),
    )

    def step(*arrays):
        return per_device(chips, *arrays)

    return jax.shard_map(
        step,
        mesh=mesh,
        in_specs=placed,
        out_specs=(P(("grp", "dp"), ("kv", "tp")), P(("grp", "dp", "kv", "tp"), None, None)),
        check_vma=False,
    )
```

```python
import functools

import jax
import jax.numpy as jnp
from jax import lax
from jax.experimental import pallas as pl
from jax.experimental.pallas import tpu as pltpu
from jax.sharding import PartitionSpec as P


epsilon = 1e-06
axes = ("kv", "tp")


def by_distance(stack, chip):
    count = stack.shape[0]
    rest = stack.shape[1:]
    bit = 1
    while bit < count:
        split = stack.reshape((count // (2 * bit), 2, bit) + rest)
        flipped = jnp.where((chip & bit) != 0, split[:, ::-1], split)
        stack = flipped.reshape((count,) + rest)
        bit *= 2
    return stack


def far(pieces, chips):
    got = [pieces[0]]
    for d in range(1, chips):
        pairs = [(i, i ^ (2 * d + 1)) for i in range(2 * chips)]
        got.append(lax.ppermute(pieces[d], axes, pairs))
    return got


def near(value):
    return lax.ppermute(value, "tp", [(0, 1), (1, 0)])


def merge(mine, other, chip, core):
    count = mine.shape[0]
    own = (jnp.arange(count) == 0).reshape((count,) + (1,) * (mine.ndim - 1))
    low_is_mine = own == (core == 0)
    low = jnp.where(low_is_mine, mine, other)
    high = jnp.where(low_is_mine, other, mine)
    both = by_distance(jnp.stack([low, high], axis=1), chip)
    return both.reshape((2 * count,) + mine.shape[1:])


def gather(piece, chips, chip, core):
    mine = jnp.stack(far([piece] * chips, chips))
    return merge(mine, near(mine), chip, core)


def gather_features(piece, chips, chip, core):
    parts = gather(piece, chips, chip, core)
    return jnp.concatenate([parts[i] for i in range(2 * chips)], axis=1)


def delta_step(queries, keys_in, values, gates, strength, log_decay, memory, head_gain):
    count = queries.shape[0]
    heads = strength.shape[1]
    size = head_gain.shape[0]
    highest = lax.Precision.HIGHEST
    query_wide = queries.astype(jnp.float32).reshape(count, heads, size)
    key_wide = keys_in.astype(jnp.float32).reshape(count, heads, size)
    value_wide = values.astype(jnp.float32).reshape(count, heads, size)
    gate_wide = gates.astype(jnp.float32).reshape(count, heads, size)
    unit_key = key_wide * lax.rsqrt(jnp.sum(key_wide * key_wide, axis=-1, keepdims=True) + epsilon)
    matrix = memory.reshape(count, heads, size, size)
    recall = jnp.einsum("bhk,bhkv->bhv", unit_key, matrix, precision=highest)
    retain = jnp.exp(log_decay)[:, :, None, None]
    scaled = strength[:, :, None]
    erased = matrix - jnp.einsum("bhk,bhv->bhkv", unit_key, scaled * recall, precision=highest)
    written = jnp.einsum("bhk,bhv->bhkv", unit_key, scaled * value_wide, precision=highest)
    updated = retain * erased + written
    readout = jnp.einsum("bhk,bhkv->bhv", query_wide, updated, precision=highest)
    normed = readout * lax.rsqrt(jnp.mean(readout * readout, axis=-1, keepdims=True) + epsilon)
    normed = normed * head_gain * jax.nn.silu(gate_wide)
    return (
        updated.reshape(count, heads, size * size),
        normed.reshape(count, heads * size).astype(jnp.bfloat16),
    )


def plain_device(
    chips,
    tokens,
    memory,
    mix_gain,
    w_query,
    w_key,
    w_value,
    w_gate,
    w_beta,
    w_decay,
    decay_rate,
    decay_bias,
    head_gain,
    w_out,
    ffn_gain,
    w_up,
    w_down,
):
    rows = tokens.shape[0]
    owned = memory.shape[0]
    width = mix_gain.shape[0]
    chip = lax.axis_index("kv")
    core = lax.axis_index("tp")
    own_start = lax.axis_index(axes) * owned
    wide = tokens.astype(jnp.float32)

    def lifted_of(whole, gain):
        whole_wide = whole.astype(jnp.float32)
        scale = lax.rsqrt(jnp.sum(whole_wide * whole_wide, axis=1) / width + epsilon)
        return (whole_wide * gain).astype(jnp.bfloat16), scale[:, None]

    def project(value, weight):
        return jnp.dot(value, weight, preferred_element_type=jnp.float32)

    lifted_in, scale_in = lifted_of(gather_features(tokens, chips, chip, core), mix_gain)
    sent = jnp.stack(
        [
            (project(lifted_in, weight) * scale_in).astype(jnp.bfloat16)
            for weight in (w_query, w_key, w_value, w_gate)
        ],
        axis=1,
    )
    strength_all = jax.nn.sigmoid(project(lifted_in, w_beta) * scale_in)
    decay_all = -decay_rate * jax.nn.softplus(project(lifted_in, w_decay) * scale_in + decay_bias)
    strength = lax.dynamic_slice_in_dim(strength_all, own_start, owned, 0)
    log_decay = lax.dynamic_slice_in_dim(decay_all, own_start, owned, 0)

    part = sent.shape[2]
    leaving = by_distance(sent.reshape(chips, 2, owned, 4, part), chip)
    mine = jnp.stack(far([leaving[d] for d in range(chips)], chips))
    other = near(mine)
    pick = lambda both: jnp.where(core == 0, both[:, 0], both[:, 1])
    whole = merge(pick(mine), pick(other), chip, core)
    whole = jnp.transpose(whole, (2, 1, 0, 3)).reshape(4, owned, 2 * chips * part)
    updated, mixed = delta_step(
        whole[0], whole[1], whole[2], whole[3], strength, log_decay, memory, head_gain
    )

    mixed_all = gather(mixed, chips, chip, core).reshape(rows, mixed.shape[1])
    middle = (wide + project(mixed_all, w_out)).astype(jnp.bfloat16)
    middle_wide = middle.astype(jnp.float32)
    lifted_mid, scale_mid = lifted_of(gather_features(middle, chips, chip, core), ffn_gain)
    raised = project(lifted_mid, w_up)
    hidden = jnp.square(jax.nn.relu(raised * scale_mid)).astype(jnp.bfloat16)
    terms = project(hidden, w_down).astype(jnp.bfloat16)

    features = tokens.shape[1]
    blocks = jnp.stack([terms[:, i * 2 * features : (i + 1) * 2 * features] for i in range(chips)])
    leaving = by_distance(blocks, chip)
    total = sum(
        (got.astype(jnp.float32) for got in far([leaving[d] for d in range(chips)], chips))
    )
    low, high = total[:, :features], total[:, features:]
    arrived = near(jnp.where(core == 0, high, low))
    down = jnp.where(core == 0, low, high) + arrived
    layer_out = (middle_wide + down).astype(jnp.bfloat16)
    return (layer_out, updated)


def place():
    return lax.axis_index("kv"), lax.axis_index("tp")


def mine_lane(d):
    chip, core = place()
    return 2 * (chip ^ d) + (core if d == 0 else 1 - core)


def other_lane(d):
    chip, core = place()
    return 2 * (chip ^ d) + (1 - core if d == 0 else core)


def span(lane, size):
    return pl.ds(pl.multiple_of(lane * size, size), size)


def dot_rows(left, right):
    return lax.dot_general(left, right, (((1,), (1,)), ((), ())), preferred_element_type=jnp.float32)


def dot(left, right):
    return jnp.dot(left, right, preferred_element_type=jnp.float32)


def call(body, outs, args, scratch=(), work=1e9):
    vmem = pl.BlockSpec(memory_space=pltpu.VMEM)
    return pl.pallas_call(
        body,
        out_shape=[jax.ShapeDtypeStruct(shape, kind) for shape, kind in outs],
        in_specs=[vmem] * len(args),
        out_specs=[vmem] * len(outs),
        scratch_shapes=list(scratch),
        compiler_params=pltpu.CompilerParams(vmem_limit_bytes=16 << 20),
        cost_estimate=pl.CostEstimate(flops=int(work), bytes_accessed=0, transcendentals=0),
    )(*args)


def keep_near(tokens, near_ref):
    near_ref[...] = tokens[...]


def project_piece(piece, lane, gain, weights, lifted, parts):
    size = piece.shape[1]
    wide = piece.astype(jnp.float32)
    ready = (wide * gain[:, span(lane, size)]).astype(jnp.bfloat16)
    lifted[:, span(lane, size)] = ready
    stacked = jnp.concatenate([weight[:, span(lane, size)] for weight in weights], axis=0)
    parts.append((dot_rows(ready, stacked), jnp.sum(wide * wide, axis=1, keepdims=True)))


def project_first(chips, tokens, partner, *refs):
    got, (gain, *rest) = refs[: chips - 1], refs[chips - 1 :]
    weights, (total, squares, lifted) = rest[:4], rest[4:]
    lifted[...] = jnp.zeros_like(lifted)
    parts = []
    project_piece(tokens[...], mine_lane(0), gain, weights, lifted, parts)
    project_piece(partner[...], other_lane(0), gain, weights, lifted, parts)
    for d in range(1, chips):
        project_piece(got[d - 1][...], mine_lane(d), gain, weights, lifted, parts)
    total[...] = sum(part[0] for part in parts)
    squares[...] = jnp.broadcast_to(sum(part[1] for part in parts), squares.shape)


def project_rest(chips, others, before, before_squares, before_lifted, gain, *rest):
    weights, (scale_ref, lifted, *leaving), sent = rest[:4], rest[4:-1], rest[-1]
    lifted[...] = before_lifted[...]
    parts = [(before[...], before_squares[:, :1])]
    for d in range(1, chips):
        project_piece(others[d - 1], other_lane(d), gain, weights, lifted, parts)
    squares = sum(part[1] for part in parts)
    scale = lax.rsqrt(squares / lifted.shape[1] + epsilon)
    total = sum(part[0] for part in parts) * scale
    sent[...] = total.astype(jnp.bfloat16).astype(jnp.float32)
    scale_ref[...] = jnp.broadcast_to(scale, scale_ref.shape)
    chip, _ = place()
    for d in range(chips):
        for c in range(2):
            leaving[d][c : c + 1, :] = sent[pl.ds(2 * (chip ^ d) + c, 1), :]


def column(row, heads):
    there = lax.broadcasted_iota(jnp.int32, (heads, heads), 0)
    here = lax.broadcasted_iota(jnp.int32, (heads, heads), 1)
    return jnp.sum(jnp.where(there == here, row, 0.0), axis=1, keepdims=True)


def own_gates(lifted, scale, w_beta, w_decay, rate, bias, strength, retain):
    heads = w_beta.shape[0]
    lane = mine_lane(0)
    scale_own = scale[pl.ds(lane, 1), :][:, :1]

    def own(weight):
        every = dot_rows(weight[...], lifted[...])
        here = lax.broadcasted_iota(jnp.int32, every.shape, 1) == lane
        return jnp.sum(jnp.where(here, every, 0.0), axis=1, keepdims=True) * scale_own

    value = own(w_decay) + column(bias[...], heads)
    soft = jnp.maximum(value, 0.0) + jnp.log1p(jnp.exp(-jnp.abs(value)))
    decay = jnp.exp(-column(rate[...], heads) * soft)
    beta = 1.0 / (1.0 + jnp.exp(-own(w_beta)))
    strength[...] = jnp.broadcast_to(beta, strength.shape)
    retain[...] = jnp.broadcast_to(decay, retain.shape)


def read_memory(chips, *refs):
    mine, other, strength, retain, memory, head_gain, mixed, turned_ref, write_ref, parts = refs
    heads, size = strength.shape
    chip, core = place()
    part = mine.shape[2] // 4
    across = 2 * part // size
    for there in range(chips):
        d = chip ^ there
        own = mine[d, pl.ds(core, 1), :]
        partner = other[d, pl.ds(core, 1), :]
        straight = (d == 0) == (core == 0)
        low = jnp.where(straight, own, partner)
        high = jnp.where(straight, partner, own)
        for t in range(4):
            cut = slice(t * part, (t + 1) * part)
            pair = jnp.concatenate([low[:, cut], high[:, cut]], axis=1)
            for i in range(across):
                h = there * across + i
                parts[t, h : h + 1, :] = pair[:, i * size : (i + 1) * size]
    query, key, value, gate = parts[0], parts[1], parts[2], parts[3]
    shrink = lax.rsqrt(jnp.sum(key * key, axis=1, keepdims=True) + epsilon)
    padded = -(-heads // 8) * 8
    pad = [jnp.zeros((padded - heads, size), jnp.float32)] if padded > heads else []
    rest = jnp.zeros((size - 2 * padded, size), jnp.float32)
    turned = jnp.concatenate([key, *pad, query, *pad, rest], axis=0).T
    recalls, reads = [], []
    for h in range(heads):
        matrix = memory[h]
        recalls.append(jnp.sum(matrix * turned[:, h : h + 1], axis=0, keepdims=True))
        at = padded + h
        reads.append(jnp.sum(matrix * turned[:, at : at + 1], axis=0, keepdims=True))
    recall = jnp.concatenate(recalls, axis=0) * shrink
    read = jnp.concatenate(reads, axis=0)
    write = shrink * strength[...] * (value - retain[...] * recall)
    readout = retain[...] * read + jnp.sum(key * query, axis=1, keepdims=True) * write
    normed = readout * lax.rsqrt(jnp.mean(readout * readout, axis=1, keepdims=True) + epsilon)
    normed = normed * head_gain[...] * (gate / (1.0 + jnp.exp(-gate)))
    normed = normed.astype(jnp.bfloat16).astype(jnp.float32)
    for h in range(heads):
        mixed[:, h * size : (h + 1) * size] = normed[h : h + 1]
    turned_ref[...] = turned
    write_ref[...] = write


def update_memory(memory, turned, write, retain, updated):
    for h in range(memory.shape[0]):
        row = slice(h, h + 1)
        updated[h] = retain[row, :] * memory[h] + turned[:, row] * write[row, :]


def by_core(own, partner):
    first = place()[1] == 0
    low, high = jnp.where(first, own, partner), jnp.where(first, partner, own)
    return jnp.concatenate([low, high], axis=-1)


def mix_out(chips, tokens, partner_tokens, own, *refs):
    got, (weight, partner_weight, half, rows, wide) = refs[: chips - 1], refs[chips - 1 :]
    for d in range(chips):
        rows[d : d + 1, :] = (got[d - 1] if d else own)[...]
    left = rows[...].astype(jnp.bfloat16)
    branch = by_core(dot(left, weight[...]), dot(left, partner_weight[...]))
    wide[...] = by_core(tokens[...].astype(jnp.float32), partner_tokens[...].astype(jnp.float32))
    for d in range(chips):
        middle = wide[pl.ds(mine_lane(d), 1), :] + branch[d : d + 1]
        half[d : d + 1, :] = middle.astype(jnp.bfloat16).astype(jnp.float32)


def join_rows(chips, half, other, block, own, rows):
    for d in range(chips):
        rows[pl.ds(mine_lane(d), 1), :] = half[d : d + 1, :]
        rows[pl.ds(other_lane(d), 1), :] = other[d : d + 1, :]
    block[...] = rows[...].astype(jnp.bfloat16)
    own[...] = rows[:, span(place()[1], own.shape[1])].astype(jnp.bfloat16)


def up_piece(piece, there, gain, weight, parts):
    size = piece.shape[1]
    wide = piece.astype(jnp.float32)
    ready = (wide * gain[:, span(there, size)]).astype(jnp.bfloat16)
    parts.append((dot(ready, weight[span(there, size), :]), jnp.sum(wide * wide, axis=1, keepdims=True)))


def up_first(block, gain, weight, total, squares):
    parts = []
    up_piece(block[...], place()[0], gain, weight, parts)
    total[...] = parts[0][0]
    squares[...] = jnp.broadcast_to(parts[0][1], squares.shape)


def up_rest(chips, *refs):
    got, rest = refs[: chips - 1], refs[chips - 1 :]
    before, before_squares, gain, weight, down, hidden_ref, leaving = rest
    parts = [(before[...], before_squares[:, :1])]
    for d in range(1, chips):
        up_piece(got[d - 1][...], place()[0] ^ d, gain, weight, parts)
    scale = lax.rsqrt(sum(part[1] for part in parts) / gain.shape[1] + epsilon)
    raised = jnp.maximum(sum(part[0] for part in parts) * scale, 0.0)
    hidden = (raised * raised).astype(jnp.bfloat16)
    hidden_ref[...] = hidden
    size = leaving.shape[2]
    for d in range(chips):
        leaving[d] = dot(hidden, down[:, span(other_lane(d), size)]).astype(jnp.bfloat16)


def down_own(chips, hidden, down, staying):
    size = staying.shape[2]
    for d in range(chips):
        staying[d] = dot(hidden[...], down[:, span(mine_lane(d), size)])


def kernel_device(
    chips,
    tokens,
    memory,
    mix_gain,
    w_query,
    w_key,
    w_value,
    w_gate,
    w_beta,
    w_decay,
    decay_rate,
    decay_bias,
    head_gain,
    w_out,
    ffn_gain,
    w_up,
    w_down,
):
    f32, bf16 = jnp.float32, jnp.bfloat16
    rows, features = tokens.shape
    width = mix_gain.shape[0]
    heads = w_beta.shape[1]
    size = head_gain.shape[0]
    units = w_up.shape[1]
    part = w_query.shape[1]

    got = far([tokens] * chips, chips)[1:]
    partner = near(tokens)
    (tokens,) = call(keep_near, [(tokens.shape, bf16)], [tokens], work=8e9)
    others = near(jnp.stack(got))
    weights = [weight.T for weight in (w_query, w_key, w_value, w_gate)]
    gain_in = mix_gain.reshape(1, width)
    total, squares, lifted = call(
        functools.partial(project_first, chips),
        [((rows, 4 * part), f32), ((rows, 128), f32), ((rows, width), bf16)],
        [tokens, partner, *got, gain_in, *weights],
    )
    scale_in, lifted, *leaving = call(
        functools.partial(project_rest, chips),
        [((rows, 128), f32), ((rows, width), bf16)] + [((2, 4 * part), f32)] * chips,
        [others, total, squares, lifted, gain_in, *weights],
        [pltpu.VMEM((rows, 4 * part), f32)],
    )
    strength, retain = call(
        own_gates,
        [((heads, size), f32)] * 2,
        [lifted, scale_in, w_beta.T, w_decay.T]
        + [value.reshape(1, heads) for value in (decay_rate, decay_bias)],
    )
    mine = jnp.stack(far(leaving, chips))
    matrix = memory.reshape(heads, size, size)
    mixed, turned, write = call(
        functools.partial(read_memory, chips),
        [((1, heads * size), f32), ((size, size), f32), ((heads, size), f32)],
        [mine, near(mine), strength, retain, matrix, head_gain.reshape(1, size)],
        [pltpu.VMEM((4, heads, size), f32)],
    )
    (updated,) = call(
        update_memory, [((heads, size, size), f32)], [matrix, turned, write, retain], work=5e8
    )

    got = far([mixed] * chips, chips)[1:]
    (half,) = call(
        functools.partial(mix_out, chips),
        [((chips, 2 * features), f32)],
        [tokens, partner, mixed, *got, w_out, near(w_out)],
        [pltpu.VMEM((chips, heads * size), f32), pltpu.VMEM((rows, 2 * features), f32)],
    )
    block, middle = call(
        functools.partial(join_rows, chips),
        [((rows, 2 * features), bf16), ((rows, features), bf16)],
        [half, near(half)],
        [pltpu.VMEM((rows, 2 * features), f32)],
    )
    got = far([block] * chips, chips)[1:]
    gain_mid = ffn_gain.reshape(1, width)
    total, squares = call(
        up_first, [((rows, units), f32), ((rows, 128), f32)], [block, gain_mid, w_up]
    )
    hidden, leaving = call(
        functools.partial(up_rest, chips),
        [((rows, units), bf16), ((chips, rows, features), bf16)],
        [*got, total, squares, gain_mid, w_up, w_down],
    )
    arrived = near(leaving)
    (staying,) = call(
        functools.partial(down_own, chips), [((chips, rows, features), f32)], [hidden, w_down]
    )
    sums = staying + arrived.astype(f32)
    terms = far([sums[0]] + [sums[d].astype(bf16) for d in range(1, chips)], chips)
    down = sum(term.astype(f32) for term in terms)
    layer_out = (middle.astype(f32) + down).astype(bf16)
    return (layer_out, updated.reshape(memory.shape))


def per_device(chips, *arrays):
    tokens, memory, head_gain = arrays[0], arrays[1], arrays[11]
    fits = (
        memory.shape[0] == 1
        and tokens.shape[0] == 2 * chips
        and tokens.shape[1] % 128 == 0
        and arrays[3].shape[1] % 16 == 0
        and 2 * arrays[3].shape[1] % head_gain.shape[0] == 0
        and head_gain.shape[0] == 128
        and memory.shape[1] <= 32
    )
    return (kernel_device if fits else plain_device)(chips, *arrays)


def solution(mesh):
    chips = mesh.shape["kv"]
    placed = (
        P(("grp", "dp"), ("kv", "tp")),
        P(("grp", "dp", "kv", "tp"), None, None),
        P(),
        P(None, ("kv", "tp")),
        P(None, ("kv", "tp")),
        P(None, ("kv", "tp")),
        P(None, ("kv", "tp")),
        P(),
        P(),
        P(),
        P(),
        P(),
        P(None, ("kv", "tp")),
        P(),
        P(None, ("kv", "tp")),
        P(("kv", "tp"), None),
    )

    def step(*arrays):
        return per_device(chips, *arrays)

    return jax.shard_map(
        step,
        mesh=mesh,
        in_specs=placed,
        out_specs=(P(("grp", "dp"), ("kv", "tp")), P(("grp", "dp", "kv", "tp"), None, None)),
        check_vma=False,
    )
```

```python
import functools

import jax
import jax.numpy as jnp
from jax import lax
from jax.experimental import pallas as pl
from jax.experimental.pallas import tpu as pltpu
from jax.sharding import PartitionSpec as P


epsilon = 1e-06
axes = ("kv", "tp")


def by_distance(stack, chip):
    count = stack.shape[0]
    rest = stack.shape[1:]
    bit = 1
    while bit < count:
        split = stack.reshape((count // (2 * bit), 2, bit) + rest)
        flipped = jnp.where((chip & bit) != 0, split[:, ::-1], split)
        stack = flipped.reshape((count,) + rest)
        bit *= 2
    return stack


def far(pieces, chips):
    got = [pieces[0]]
    for d in range(1, chips):
        pairs = [(i, i ^ (2 * d + 1)) for i in range(2 * chips)]
        got.append(lax.ppermute(pieces[d], axes, pairs))
    return got


def near(value):
    return lax.ppermute(value, "tp", [(0, 1), (1, 0)])


def merge(mine, other, chip, core):
    count = mine.shape[0]
    own = (jnp.arange(count) == 0).reshape((count,) + (1,) * (mine.ndim - 1))
    low_is_mine = own == (core == 0)
    low = jnp.where(low_is_mine, mine, other)
    high = jnp.where(low_is_mine, other, mine)
    both = by_distance(jnp.stack([low, high], axis=1), chip)
    return both.reshape((2 * count,) + mine.shape[1:])


def gather(piece, chips, chip, core):
    mine = jnp.stack(far([piece] * chips, chips))
    return merge(mine, near(mine), chip, core)


def gather_features(piece, chips, chip, core):
    parts = gather(piece, chips, chip, core)
    return jnp.concatenate([parts[i] for i in range(2 * chips)], axis=1)


def delta_step(queries, keys_in, values, gates, strength, log_decay, memory, head_gain):
    count = queries.shape[0]
    heads = strength.shape[1]
    size = head_gain.shape[0]
    highest = lax.Precision.HIGHEST
    query_wide = queries.astype(jnp.float32).reshape(count, heads, size)
    key_wide = keys_in.astype(jnp.float32).reshape(count, heads, size)
    value_wide = values.astype(jnp.float32).reshape(count, heads, size)
    gate_wide = gates.astype(jnp.float32).reshape(count, heads, size)
    unit_key = key_wide * lax.rsqrt(jnp.sum(key_wide * key_wide, axis=-1, keepdims=True) + epsilon)
    matrix = memory.reshape(count, heads, size, size)
    recall = jnp.einsum("bhk,bhkv->bhv", unit_key, matrix, precision=highest)
    retain = jnp.exp(log_decay)[:, :, None, None]
    scaled = strength[:, :, None]
    erased = matrix - jnp.einsum("bhk,bhv->bhkv", unit_key, scaled * recall, precision=highest)
    written = jnp.einsum("bhk,bhv->bhkv", unit_key, scaled * value_wide, precision=highest)
    updated = retain * erased + written
    readout = jnp.einsum("bhk,bhkv->bhv", query_wide, updated, precision=highest)
    normed = readout * lax.rsqrt(jnp.mean(readout * readout, axis=-1, keepdims=True) + epsilon)
    normed = normed * head_gain * jax.nn.silu(gate_wide)
    return (
        updated.reshape(count, heads, size * size),
        normed.reshape(count, heads * size).astype(jnp.bfloat16),
    )


def plain_device(
    chips,
    tokens,
    memory,
    mix_gain,
    w_query,
    w_key,
    w_value,
    w_gate,
    w_beta,
    w_decay,
    decay_rate,
    decay_bias,
    head_gain,
    w_out,
    ffn_gain,
    w_up,
    w_down,
):
    rows = tokens.shape[0]
    owned = memory.shape[0]
    width = mix_gain.shape[0]
    chip = lax.axis_index("kv")
    core = lax.axis_index("tp")
    own_start = lax.axis_index(axes) * owned
    wide = tokens.astype(jnp.float32)

    def lifted_of(whole, gain):
        whole_wide = whole.astype(jnp.float32)
        scale = lax.rsqrt(jnp.sum(whole_wide * whole_wide, axis=1) / width + epsilon)
        return (whole_wide * gain).astype(jnp.bfloat16), scale[:, None]

    def project(value, weight):
        return jnp.dot(value, weight, preferred_element_type=jnp.float32)

    lifted_in, scale_in = lifted_of(gather_features(tokens, chips, chip, core), mix_gain)
    sent = jnp.stack(
        [
            (project(lifted_in, weight) * scale_in).astype(jnp.bfloat16)
            for weight in (w_query, w_key, w_value, w_gate)
        ],
        axis=1,
    )
    strength_all = jax.nn.sigmoid(project(lifted_in, w_beta) * scale_in)
    decay_all = -decay_rate * jax.nn.softplus(project(lifted_in, w_decay) * scale_in + decay_bias)
    strength = lax.dynamic_slice_in_dim(strength_all, own_start, owned, 0)
    log_decay = lax.dynamic_slice_in_dim(decay_all, own_start, owned, 0)

    part = sent.shape[2]
    leaving = by_distance(sent.reshape(chips, 2, owned, 4, part), chip)
    mine = jnp.stack(far([leaving[d] for d in range(chips)], chips))
    other = near(mine)
    pick = lambda both: jnp.where(core == 0, both[:, 0], both[:, 1])
    whole = merge(pick(mine), pick(other), chip, core)
    whole = jnp.transpose(whole, (2, 1, 0, 3)).reshape(4, owned, 2 * chips * part)
    updated, mixed = delta_step(
        whole[0], whole[1], whole[2], whole[3], strength, log_decay, memory, head_gain
    )

    mixed_all = gather(mixed, chips, chip, core).reshape(rows, mixed.shape[1])
    middle = (wide + project(mixed_all, w_out)).astype(jnp.bfloat16)
    middle_wide = middle.astype(jnp.float32)
    lifted_mid, scale_mid = lifted_of(gather_features(middle, chips, chip, core), ffn_gain)
    raised = project(lifted_mid, w_up)
    hidden = jnp.square(jax.nn.relu(raised * scale_mid)).astype(jnp.bfloat16)
    terms = project(hidden, w_down).astype(jnp.bfloat16)

    features = tokens.shape[1]
    blocks = jnp.stack([terms[:, i * 2 * features : (i + 1) * 2 * features] for i in range(chips)])
    leaving = by_distance(blocks, chip)
    total = sum(
        (got.astype(jnp.float32) for got in far([leaving[d] for d in range(chips)], chips))
    )
    low, high = total[:, :features], total[:, features:]
    arrived = near(jnp.where(core == 0, high, low))
    down = jnp.where(core == 0, low, high) + arrived
    layer_out = (middle_wide + down).astype(jnp.bfloat16)
    return (layer_out, updated)


def place():
    return lax.axis_index("kv"), lax.axis_index("tp")


def mine_lane(d):
    chip, core = place()
    return 2 * (chip ^ d) + (core if d == 0 else 1 - core)


def other_lane(d):
    chip, core = place()
    return 2 * (chip ^ d) + (1 - core if d == 0 else core)


def span(lane, size):
    return pl.ds(pl.multiple_of(lane * size, size), size)


def dot_rows(left, right):
    return lax.dot_general(left, right, (((1,), (1,)), ((), ())), preferred_element_type=jnp.float32)


def dot(left, right):
    return jnp.dot(left, right, preferred_element_type=jnp.float32)


def call(body, outs, args, scratch=(), work=1e9):
    vmem = pl.BlockSpec(memory_space=pltpu.VMEM)
    return pl.pallas_call(
        body,
        out_shape=[jax.ShapeDtypeStruct(shape, kind) for shape, kind in outs],
        in_specs=[vmem] * len(args),
        out_specs=[vmem] * len(outs),
        scratch_shapes=list(scratch),
        compiler_params=pltpu.CompilerParams(vmem_limit_bytes=16 << 20),
        cost_estimate=pl.CostEstimate(flops=int(work), bytes_accessed=0, transcendentals=0),
    )(*args)


def keep_near(tokens, near_ref):
    near_ref[...] = tokens[...]


def project_piece(piece, lane, gain, weights, lifted, parts):
    size = piece.shape[1]
    wide = piece.astype(jnp.float32)
    ready = (wide * gain[:, span(lane, size)]).astype(jnp.bfloat16)
    lifted[:, span(lane, size)] = ready
    stacked = jnp.concatenate([weight[:, span(lane, size)] for weight in weights], axis=0)
    parts.append((dot_rows(ready, stacked), jnp.sum(wide * wide, axis=1, keepdims=True)))


def project_first(chips, tokens, partner, *refs):
    got, (gain, *rest) = refs[: chips - 1], refs[chips - 1 :]
    weights, (total, squares, lifted) = rest[:4], rest[4:]
    lifted[...] = jnp.zeros_like(lifted)
    parts = []
    project_piece(tokens[...], mine_lane(0), gain, weights, lifted, parts)
    project_piece(partner[...], other_lane(0), gain, weights, lifted, parts)
    for d in range(1, chips):
        project_piece(got[d - 1][...], mine_lane(d), gain, weights, lifted, parts)
    total[...] = sum(part[0] for part in parts)
    squares[...] = jnp.broadcast_to(sum(part[1] for part in parts), squares.shape)


def project_rest(chips, others, before, before_squares, before_lifted, gain, *rest):
    weights, (scale_ref, lifted, *leaving), sent = rest[:4], rest[4:-1], rest[-1]
    lifted[...] = before_lifted[...]
    parts = [(before[...], before_squares[:, :1])]
    for d in range(1, chips):
        project_piece(others[d - 1], other_lane(d), gain, weights, lifted, parts)
    squares = sum(part[1] for part in parts)
    scale = lax.rsqrt(squares / lifted.shape[1] + epsilon)
    total = sum(part[0] for part in parts) * scale
    sent[...] = total.astype(jnp.bfloat16).astype(jnp.float32)
    scale_ref[...] = jnp.broadcast_to(scale, scale_ref.shape)
    chip, _ = place()
    for d in range(chips):
        for c in range(2):
            leaving[d][c : c + 1, :] = sent[pl.ds(2 * (chip ^ d) + c, 1), :]


def column(row, heads):
    there = lax.broadcasted_iota(jnp.int32, (heads, heads), 0)
    here = lax.broadcasted_iota(jnp.int32, (heads, heads), 1)
    return jnp.sum(jnp.where(there == here, row, 0.0), axis=1, keepdims=True)


def gates(lifted, scale, w_beta, w_decay, rate, bias, *outs):
    heads = w_beta.shape[0]
    beta_all, decay_all = dot_rows(w_beta[...], lifted[...]), dot_rows(w_decay[...], lifted[...])
    bias_column, rate_column = column(bias[...], heads), column(rate[...], heads)
    for lane, (strength, retain) in ((mine_lane(0), outs[:2]), (other_lane(0), outs[2:])):
        scale_own = scale[pl.ds(lane, 1), :][:, :1]
        here = lax.broadcasted_iota(jnp.int32, beta_all.shape, 1) == lane

        def own(every):
            return jnp.sum(jnp.where(here, every, 0.0), axis=1, keepdims=True) * scale_own

        value = own(decay_all) + bias_column
        soft = jnp.maximum(value, 0.0) + jnp.log1p(jnp.exp(-jnp.abs(value)))
        decay = jnp.exp(-rate_column * soft)
        beta = 1.0 / (1.0 + jnp.exp(-own(beta_all)))
        strength[...] = jnp.broadcast_to(beta, strength.shape)
        retain[...] = jnp.broadcast_to(decay, retain.shape)


def read_row(chips, row, mine, other, strength, retain, terms, head_gain, parts):
    heads, size = strength.shape
    chip, core = place()
    part = mine.shape[2] // 4
    across = 2 * part // size
    for there in range(chips):
        d = chip ^ there
        own = mine[d, pl.ds(row, 1), :]
        partner = other[d, pl.ds(row, 1), :]
        straight = (d == 0) == (core == 0)
        low = jnp.where(straight, own, partner)
        high = jnp.where(straight, partner, own)
        for t in range(4):
            cut = slice(t * part, (t + 1) * part)
            pair = jnp.concatenate([low[:, cut], high[:, cut]], axis=1)
            for i in range(across):
                h = there * across + i
                parts[t, h : h + 1, :] = pair[:, i * size : (i + 1) * size]
    query, key, value, gate = parts[0], parts[1], parts[2], parts[3]
    shrink = lax.rsqrt(jnp.sum(key * key, axis=1, keepdims=True) + epsilon)
    padded = -(-heads // 16) * 16
    pad = [jnp.zeros((padded - heads, size), jnp.float32)] if padded > heads else []
    left = jnp.concatenate([key, *pad, query, *pad], axis=0).astype(jnp.bfloat16)
    at = lax.rem(lax.broadcasted_iota(jnp.int32, (2 * padded, 3 * size), 0), padded)
    found = sum(jnp.where(at == h, dot(left, terms[h]), 0.0) for h in range(heads))
    found = found[:, :size] + found[:, size : 2 * size] + found[:, 2 * size :]
    recall, read = found[:heads] * shrink, found[padded : padded + heads]
    write = shrink * strength[...] * (value - retain[...] * recall)
    readout = retain[...] * read + jnp.sum(key * query, axis=1, keepdims=True) * write
    normed = readout * lax.rsqrt(jnp.mean(readout * readout, axis=1, keepdims=True) + epsilon)
    normed = normed * head_gain[...] * (gate / (1.0 + jnp.exp(-gate)))
    return normed.astype(jnp.bfloat16).astype(jnp.float32), key, write


def read_memory(chips, mine, other, *refs):
    outer, (head_gain, mixed, key_ref, write_ref, parts) = refs[:6], refs[6:]
    heads, size = key_ref.shape
    _, core = place()
    given = ((core, outer[0:3]), (1 - core, outer[3:6]))
    rows = [
        read_row(chips, row, mine, other, *three, head_gain, parts.at[i])
        for i, (row, three) in enumerate(given)
    ]
    own, partner = rows[0][0], rows[1][0]
    ordered = jnp.where(core == 0, own, partner), jnp.where(core == 0, partner, own)
    for h in range(heads):
        for c in range(2):
            mixed[c : c + 1, h * size : (h + 1) * size] = ordered[c][h : h + 1]
    key_ref[...] = rows[0][1]
    write_ref[...] = rows[0][2]


def split_memory(memory, terms):
    size = memory.shape[2]
    for h in range(memory.shape[0]):
        left = memory[h]
        for i in range(3):
            term = left.astype(jnp.bfloat16)
            terms[h, :, i * size : (i + 1) * size] = term
            left = left - term.astype(jnp.float32)


def update_memory(memory, key, write, retain, updated):
    heads, size = key.shape
    rest = jnp.zeros((size - heads, size), jnp.float32)
    turned = jnp.concatenate([key[...], rest], axis=0).T
    for h in range(heads):
        row = slice(h, h + 1)
        updated[h] = retain[row, :] * memory[h] + turned[:, row] * write[row, :]


def by_core(own, partner):
    first = place()[1] == 0
    low, high = jnp.where(first, own, partner), jnp.where(first, partner, own)
    return jnp.concatenate([low, high], axis=-1)


def mix_out(chips, tokens, partner_tokens, own, *refs):
    got, (weight, partner_weight, block, middle, rows, wide) = refs[: chips - 1], refs[chips - 1 :]
    chip, core = place()
    for d in range(chips):
        for c in range(2):
            rows[pl.ds(2 * (chip ^ d) + c, 1), :] = (got[d - 1] if d else own)[c : c + 1, :]
    left = rows[...].astype(jnp.bfloat16)
    branch = by_core(dot(left, weight[...]), dot(left, partner_weight[...]))
    whole = branch + by_core(tokens[...].astype(jnp.float32), partner_tokens[...].astype(jnp.float32))
    block[...] = whole.astype(jnp.bfloat16)
    wide[...] = whole
    middle[...] = wide[:, span(core, middle.shape[1])].astype(jnp.bfloat16)


def up_piece(piece, there, gain, weight, parts):
    size = piece.shape[1]
    wide = piece.astype(jnp.float32)
    ready = (wide * gain[:, span(there, size)]).astype(jnp.bfloat16)
    parts.append((dot(ready, weight[span(there, size), :]), jnp.sum(wide * wide, axis=1, keepdims=True)))


def up_first(chips, block, farthest, gain, weight, total, squares):
    parts = []
    up_piece(block[...], place()[0], gain, weight, parts)
    up_piece(farthest[...], place()[0] ^ (chips - 1), gain, weight, parts)
    total[...] = sum(part[0] for part in parts)
    squares[...] = jnp.broadcast_to(sum(part[1] for part in parts), squares.shape)


def up_rest(chips, *refs):
    got, rest = refs[: chips - 2], refs[chips - 2 :]
    before, before_squares, gain, weight, down, hidden_ref, leaving = rest
    parts = [(before[...], before_squares[:, :1])]
    for d in range(1, chips - 1):
        up_piece(got[d - 1][...], place()[0] ^ d, gain, weight, parts)
    scale = lax.rsqrt(sum(part[1] for part in parts) / gain.shape[1] + epsilon)
    raised = jnp.maximum(sum(part[0] for part in parts) * scale, 0.0)
    hidden = (raised * raised).astype(jnp.bfloat16)
    hidden_ref[...] = hidden
    size = leaving.shape[2]
    for d in range(chips):
        leaving[d] = dot(hidden, down[:, span(other_lane(d), size)]).astype(jnp.bfloat16)


def down_own(chips, hidden, down, staying):
    size = staying.shape[2]
    for d in range(chips):
        staying[d] = dot(hidden[...], down[:, span(mine_lane(d), size)])


def kernel_device(
    chips,
    tokens,
    memory,
    mix_gain,
    w_query,
    w_key,
    w_value,
    w_gate,
    w_beta,
    w_decay,
    decay_rate,
    decay_bias,
    head_gain,
    w_out,
    ffn_gain,
    w_up,
    w_down,
):
    f32, bf16 = jnp.float32, jnp.bfloat16
    rows, features = tokens.shape
    width = mix_gain.shape[0]
    heads = w_beta.shape[1]
    size = head_gain.shape[0]
    units = w_up.shape[1]
    part = w_query.shape[1]

    got = far([tokens] * chips, chips)[1:]
    partner = near(tokens)
    (tokens,) = call(keep_near, [(tokens.shape, bf16)], [tokens], work=8e9)
    others = near(jnp.stack(got))
    weights = [weight.T for weight in (w_query, w_key, w_value, w_gate)]
    gain_in = mix_gain.reshape(1, width)
    total, squares, lifted = call(
        functools.partial(project_first, chips),
        [((rows, 4 * part), f32), ((rows, 128), f32), ((rows, width), bf16)],
        [tokens, partner, *got, gain_in, *weights],
    )
    scale_in, lifted, *leaving = call(
        functools.partial(project_rest, chips),
        [((rows, 128), f32), ((rows, width), bf16)] + [((2, 4 * part), f32)] * chips,
        [others, total, squares, lifted, gain_in, *weights],
        [pltpu.VMEM((rows, 4 * part), f32)],
    )
    strength, retain, partner_strength, partner_retain = call(
        gates,
        [((heads, size), f32)] * 4,
        [lifted, scale_in, w_beta.T, w_decay.T]
        + [value.reshape(1, heads) for value in (decay_rate, decay_bias)],
    )
    mine = jnp.stack(far(leaving, chips))
    matrix = memory.reshape(heads, size, size)
    shape = ((heads, size, 3 * size), bf16)
    (terms,) = call(split_memory, [shape], [matrix], work=5e8)
    (partner_terms,) = call(split_memory, [shape], [near(matrix)], work=5e8)
    mixed, key, write = call(
        functools.partial(read_memory, chips),
        [((2, heads * size), f32), ((heads, size), f32), ((heads, size), f32)],
        [mine, near(mine), strength, retain, terms, partner_strength, partner_retain, partner_terms]
        + [head_gain.reshape(1, size)],
        [pltpu.VMEM((2, 4, heads, size), f32)],
    )
    (updated,) = call(
        update_memory, [((heads, size, size), f32)], [matrix, key, write, retain], work=5e8
    )

    got = far([mixed] * chips, chips)[1:]
    block, middle = call(
        functools.partial(mix_out, chips),
        [((rows, 2 * features), bf16), ((rows, features), bf16)],
        [tokens, partner, mixed, *got, w_out, near(w_out)],
        [pltpu.VMEM((rows, heads * size), f32), pltpu.VMEM((rows, 2 * features), f32)],
    )
    got = far([block] * chips, chips)[1:]
    gain_mid = ffn_gain.reshape(1, width)
    total, squares = call(
        functools.partial(up_first, chips),
        [((rows, units), f32), ((rows, 128), f32)],
        [block, got[-1], gain_mid, w_up],
    )
    hidden, leaving = call(
        functools.partial(up_rest, chips),
        [((rows, units), bf16), ((chips, rows, features), bf16)],
        [*got[:-1], total, squares, gain_mid, w_up, w_down],
    )
    arrived = near(leaving)
    (staying,) = call(
        functools.partial(down_own, chips), [((chips, rows, features), f32)], [hidden, w_down]
    )
    sums = staying + arrived.astype(f32)
    terms = far([sums[0]] + [sums[d].astype(bf16) for d in range(1, chips)], chips)
    down = sum(term.astype(f32) for term in terms)
    layer_out = (middle.astype(f32) + down).astype(bf16)
    return (layer_out, updated.reshape(memory.shape))


def per_device(chips, *arrays):
    tokens, memory, head_gain = arrays[0], arrays[1], arrays[11]
    fits = (
        memory.shape[0] == 1
        and tokens.shape[0] == 2 * chips
        and tokens.shape[1] % 128 == 0
        and arrays[3].shape[1] % 16 == 0
        and 2 * arrays[3].shape[1] % head_gain.shape[0] == 0
        and head_gain.shape[0] == 128
        and memory.shape[1] <= 128
    )
    return (kernel_device if fits else plain_device)(chips, *arrays)


def solution(mesh):
    chips = mesh.shape["kv"]
    placed = (
        P(("grp", "dp"), ("kv", "tp")),
        P(("grp", "dp", "kv", "tp"), None, None),
        P(),
        P(None, ("kv", "tp")),
        P(None, ("kv", "tp")),
        P(None, ("kv", "tp")),
        P(None, ("kv", "tp")),
        P(),
        P(),
        P(),
        P(),
        P(),
        P(None, ("kv", "tp")),
        P(),
        P(None, ("kv", "tp")),
        P(("kv", "tp"), None),
    )

    def step(*arrays):
        return per_device(chips, *arrays)

    return jax.shard_map(
        step,
        mesh=mesh,
        in_specs=placed,
        out_specs=(P(("grp", "dp"), ("kv", "tp")), P(("grp", "dp", "kv", "tp"), None, None)),
        check_vma=False,
    )
```

```python
import functools

import jax
import jax.numpy as jnp
from jax import lax
from jax.experimental import pallas as pl
from jax.experimental.pallas import tpu as pltpu
from jax.sharding import PartitionSpec as P


epsilon = 1e-06
axes = ("kv", "tp")


def by_distance(stack, chip):
    count = stack.shape[0]
    rest = stack.shape[1:]
    bit = 1
    while bit < count:
        split = stack.reshape((count // (2 * bit), 2, bit) + rest)
        flipped = jnp.where((chip & bit) != 0, split[:, ::-1], split)
        stack = flipped.reshape((count,) + rest)
        bit *= 2
    return stack


def far(pieces, chips):
    got = [pieces[0]]
    for d in range(1, chips):
        pairs = [(i, i ^ (2 * d + 1)) for i in range(2 * chips)]
        got.append(lax.ppermute(pieces[d], axes, pairs))
    return got


def shared(piece, chips):
    falling = list(range(chips - 1, 0, -1))
    direct, passed = [], []
    for at in range(0, len(falling), 2):
        far_one, less = falling[at], falling[min(at + 1, len(falling) - 1)]
        pairs = [(i, i ^ (2 * (far_one if i % 2 else less))) for i in range(2 * chips)]
        got = lax.ppermute(piece, axes, pairs)
        direct.append((got, (less, far_one)))
        if less != far_one:
            passed.append((near(got), (far_one, less)))
    return direct, passed


def near(value):
    return lax.ppermute(value, "tp", [(0, 1), (1, 0)])


def merge(mine, other, chip, core):
    count = mine.shape[0]
    own = (jnp.arange(count) == 0).reshape((count,) + (1,) * (mine.ndim - 1))
    low_is_mine = own == (core == 0)
    low = jnp.where(low_is_mine, mine, other)
    high = jnp.where(low_is_mine, other, mine)
    both = by_distance(jnp.stack([low, high], axis=1), chip)
    return both.reshape((2 * count,) + mine.shape[1:])


def gather(piece, chips, chip, core):
    mine = jnp.stack(far([piece] * chips, chips))
    return merge(mine, near(mine), chip, core)


def gather_features(piece, chips, chip, core):
    parts = gather(piece, chips, chip, core)
    return jnp.concatenate([parts[i] for i in range(2 * chips)], axis=1)


def delta_step(queries, keys_in, values, gates, strength, log_decay, memory, head_gain):
    count = queries.shape[0]
    heads = strength.shape[1]
    size = head_gain.shape[0]
    highest = lax.Precision.HIGHEST
    query_wide = queries.astype(jnp.float32).reshape(count, heads, size)
    key_wide = keys_in.astype(jnp.float32).reshape(count, heads, size)
    value_wide = values.astype(jnp.float32).reshape(count, heads, size)
    gate_wide = gates.astype(jnp.float32).reshape(count, heads, size)
    unit_key = key_wide * lax.rsqrt(jnp.sum(key_wide * key_wide, axis=-1, keepdims=True) + epsilon)
    matrix = memory.reshape(count, heads, size, size)
    recall = jnp.einsum("bhk,bhkv->bhv", unit_key, matrix, precision=highest)
    retain = jnp.exp(log_decay)[:, :, None, None]
    scaled = strength[:, :, None]
    erased = matrix - jnp.einsum("bhk,bhv->bhkv", unit_key, scaled * recall, precision=highest)
    written = jnp.einsum("bhk,bhv->bhkv", unit_key, scaled * value_wide, precision=highest)
    updated = retain * erased + written
    readout = jnp.einsum("bhk,bhkv->bhv", query_wide, updated, precision=highest)
    normed = readout * lax.rsqrt(jnp.mean(readout * readout, axis=-1, keepdims=True) + epsilon)
    normed = normed * head_gain * jax.nn.silu(gate_wide)
    return (
        updated.reshape(count, heads, size * size),
        normed.reshape(count, heads * size).astype(jnp.bfloat16),
    )


def plain_device(
    chips,
    tokens,
    memory,
    mix_gain,
    w_query,
    w_key,
    w_value,
    w_gate,
    w_beta,
    w_decay,
    decay_rate,
    decay_bias,
    head_gain,
    w_out,
    ffn_gain,
    w_up,
    w_down,
):
    rows = tokens.shape[0]
    owned = memory.shape[0]
    width = mix_gain.shape[0]
    chip = lax.axis_index("kv")
    core = lax.axis_index("tp")
    own_start = lax.axis_index(axes) * owned
    wide = tokens.astype(jnp.float32)

    def lifted_of(whole, gain):
        whole_wide = whole.astype(jnp.float32)
        scale = lax.rsqrt(jnp.sum(whole_wide * whole_wide, axis=1) / width + epsilon)
        return (whole_wide * gain).astype(jnp.bfloat16), scale[:, None]

    def project(value, weight):
        return jnp.dot(value, weight, preferred_element_type=jnp.float32)

    lifted_in, scale_in = lifted_of(gather_features(tokens, chips, chip, core), mix_gain)
    sent = jnp.stack(
        [
            (project(lifted_in, weight) * scale_in).astype(jnp.bfloat16)
            for weight in (w_query, w_key, w_value, w_gate)
        ],
        axis=1,
    )
    strength_all = jax.nn.sigmoid(project(lifted_in, w_beta) * scale_in)
    decay_all = -decay_rate * jax.nn.softplus(project(lifted_in, w_decay) * scale_in + decay_bias)
    strength = lax.dynamic_slice_in_dim(strength_all, own_start, owned, 0)
    log_decay = lax.dynamic_slice_in_dim(decay_all, own_start, owned, 0)

    part = sent.shape[2]
    leaving = by_distance(sent.reshape(chips, 2, owned, 4, part), chip)
    mine = jnp.stack(far([leaving[d] for d in range(chips)], chips))
    other = near(mine)
    pick = lambda both: jnp.where(core == 0, both[:, 0], both[:, 1])
    whole = merge(pick(mine), pick(other), chip, core)
    whole = jnp.transpose(whole, (2, 1, 0, 3)).reshape(4, owned, 2 * chips * part)
    updated, mixed = delta_step(
        whole[0], whole[1], whole[2], whole[3], strength, log_decay, memory, head_gain
    )

    mixed_all = gather(mixed, chips, chip, core).reshape(rows, mixed.shape[1])
    middle = (wide + project(mixed_all, w_out)).astype(jnp.bfloat16)
    middle_wide = middle.astype(jnp.float32)
    lifted_mid, scale_mid = lifted_of(gather_features(middle, chips, chip, core), ffn_gain)
    raised = project(lifted_mid, w_up)
    hidden = jnp.square(jax.nn.relu(raised * scale_mid)).astype(jnp.bfloat16)
    terms = project(hidden, w_down).astype(jnp.bfloat16)

    features = tokens.shape[1]
    blocks = jnp.stack([terms[:, i * 2 * features : (i + 1) * 2 * features] for i in range(chips)])
    leaving = by_distance(blocks, chip)
    total = sum(
        (got.astype(jnp.float32) for got in far([leaving[d] for d in range(chips)], chips))
    )
    low, high = total[:, :features], total[:, features:]
    arrived = near(jnp.where(core == 0, high, low))
    down = jnp.where(core == 0, low, high) + arrived
    layer_out = (middle_wide + down).astype(jnp.bfloat16)
    return (layer_out, updated)


def place():
    return lax.axis_index("kv"), lax.axis_index("tp")


def mine_lane(d):
    chip, core = place()
    return 2 * (chip ^ d) + (core if d == 0 else 1 - core)


def other_lane(d):
    chip, core = place()
    return 2 * (chip ^ d) + (1 - core if d == 0 else core)


def span(lane, size):
    return pl.ds(pl.multiple_of(lane * size, size), size)


def dot_rows(left, right):
    return lax.dot_general(left, right, (((1,), (1,)), ((), ())), preferred_element_type=jnp.float32)


def dot(left, right):
    return jnp.dot(left, right, preferred_element_type=jnp.float32)


def call(body, outs, args, scratch=(), work=1e9):
    vmem = pl.BlockSpec(memory_space=pltpu.VMEM)
    return pl.pallas_call(
        body,
        out_shape=[jax.ShapeDtypeStruct(shape, kind) for shape, kind in outs],
        in_specs=[vmem] * len(args),
        out_specs=[vmem] * len(outs),
        scratch_shapes=list(scratch),
        compiler_params=pltpu.CompilerParams(vmem_limit_bytes=16 << 20),
        cost_estimate=pl.CostEstimate(flops=int(work), bytes_accessed=0, transcendentals=0),
    )(*args)


def keep_near(tokens, near_ref):
    near_ref[...] = tokens[...]


def project_piece(piece, lane, gain, weights, lifted, parts):
    size = piece.shape[1]
    wide = piece.astype(jnp.float32)
    ready = (wide * gain[:, span(lane, size)]).astype(jnp.bfloat16)
    lifted[:, span(lane, size)] = ready
    stacked = jnp.concatenate([weight[:, span(lane, size)] for weight in weights], axis=0)
    parts.append((dot_rows(ready, stacked), jnp.sum(wide * wide, axis=1, keepdims=True)))


def project_first(chips, tokens, partner, *refs):
    got, (gain, *rest) = refs[: chips - 1], refs[chips - 1 :]
    weights, (total, squares, lifted) = rest[:4], rest[4:]
    lifted[...] = jnp.zeros_like(lifted)
    parts = []
    project_piece(tokens[...], mine_lane(0), gain, weights, lifted, parts)
    project_piece(partner[...], other_lane(0), gain, weights, lifted, parts)
    for d in range(1, chips):
        project_piece(got[d - 1][...], mine_lane(d), gain, weights, lifted, parts)
    total[...] = sum(part[0] for part in parts)
    squares[...] = jnp.broadcast_to(sum(part[1] for part in parts), squares.shape)


def project_rest(chips, others, before, before_squares, before_lifted, gain, *rest):
    weights, (scale_ref, lifted, *leaving), sent = rest[:4], rest[4:-1], rest[-1]
    lifted[...] = before_lifted[...]
    parts = [(before[...], before_squares[:, :1])]
    for d in range(1, chips):
        project_piece(others[d - 1], other_lane(d), gain, weights, lifted, parts)
    squares = sum(part[1] for part in parts)
    scale = lax.rsqrt(squares / lifted.shape[1] + epsilon)
    total = sum(part[0] for part in parts) * scale
    sent[...] = total.astype(jnp.bfloat16).astype(jnp.float32)
    scale_ref[...] = jnp.broadcast_to(scale, scale_ref.shape)
    chip, _ = place()
    for d in range(chips):
        for c in range(2):
            leaving[d][c : c + 1, :] = sent[pl.ds(2 * (chip ^ d) + c, 1), :]


def column(row, heads):
    there = lax.broadcasted_iota(jnp.int32, (heads, heads), 0)
    here = lax.broadcasted_iota(jnp.int32, (heads, heads), 1)
    return jnp.sum(jnp.where(there == here, row, 0.0), axis=1, keepdims=True)


def gates(lifted, scale, w_beta, w_decay, rate, bias, *outs):
    heads = w_beta.shape[0]
    beta_all, decay_all = dot_rows(w_beta[...], lifted[...]), dot_rows(w_decay[...], lifted[...])
    bias_column, rate_column = column(bias[...], heads), column(rate[...], heads)
    for lane, (strength, retain) in ((mine_lane(0), outs[:2]), (other_lane(0), outs[2:])):
        scale_own = scale[pl.ds(lane, 1), :][:, :1]
        here = lax.broadcasted_iota(jnp.int32, beta_all.shape, 1) == lane

        def own(every):
            return jnp.sum(jnp.where(here, every, 0.0), axis=1, keepdims=True) * scale_own

        value = own(decay_all) + bias_column
        soft = jnp.maximum(value, 0.0) + jnp.log1p(jnp.exp(-jnp.abs(value)))
        decay = jnp.exp(-rate_column * soft)
        beta = 1.0 / (1.0 + jnp.exp(-own(beta_all)))
        strength[...] = jnp.broadcast_to(beta, strength.shape)
        retain[...] = jnp.broadcast_to(decay, retain.shape)


def read_row(chips, row, mine, other, strength, retain, terms, head_gain, parts):
    heads, size = strength.shape
    chip, core = place()
    part = mine.shape[2] // 4
    across = 2 * part // size
    for there in range(chips):
        d = chip ^ there
        own = mine[d, pl.ds(row, 1), :]
        partner = other[d, pl.ds(row, 1), :]
        straight = (d == 0) == (core == 0)
        low = jnp.where(straight, own, partner)
        high = jnp.where(straight, partner, own)
        for t in range(4):
            cut = slice(t * part, (t + 1) * part)
            pair = jnp.concatenate([low[:, cut], high[:, cut]], axis=1)
            for i in range(across):
                h = there * across + i
                parts[t, h : h + 1, :] = pair[:, i * size : (i + 1) * size]
    query, key, value, gate = parts[0], parts[1], parts[2], parts[3]
    shrink = lax.rsqrt(jnp.sum(key * key, axis=1, keepdims=True) + epsilon)
    padded = -(-heads // 16) * 16
    pad = [jnp.zeros((padded - heads, size), jnp.float32)] if padded > heads else []
    left = jnp.concatenate([key, *pad, query, *pad], axis=0).astype(jnp.bfloat16)
    at = lax.rem(lax.broadcasted_iota(jnp.int32, (2 * padded, 2 * size), 0), padded)
    found = sum(jnp.where(at == h, dot(left, terms[h]), 0.0) for h in range(heads))
    found = found[:, :size] + found[:, size:]
    recall, read = found[:heads] * shrink, found[padded : padded + heads]
    write = shrink * strength[...] * (value - retain[...] * recall)
    readout = retain[...] * read + jnp.sum(key * query, axis=1, keepdims=True) * write
    normed = readout * lax.rsqrt(jnp.mean(readout * readout, axis=1, keepdims=True) + epsilon)
    normed = normed * head_gain[...] * (gate / (1.0 + jnp.exp(-gate)))
    return normed.astype(jnp.bfloat16).astype(jnp.float32), key, write


def read_memory(chips, mine, other, *refs):
    outer, (head_gain, mixed, key_ref, write_ref, parts) = refs[:6], refs[6:]
    heads, size = key_ref.shape
    _, core = place()
    given = ((core, outer[0:3]), (1 - core, outer[3:6]))
    rows = [
        read_row(chips, row, mine, other, *three, head_gain, parts.at[i])
        for i, (row, three) in enumerate(given)
    ]
    own, partner = rows[0][0], rows[1][0]
    ordered = jnp.where(core == 0, own, partner), jnp.where(core == 0, partner, own)
    for h in range(heads):
        for c in range(2):
            mixed[c : c + 1, h * size : (h + 1) * size] = ordered[c][h : h + 1]
    key_ref[...] = rows[0][1]
    write_ref[...] = rows[0][2]


def split_memory(memory, terms):
    size = memory.shape[2]
    for h in range(memory.shape[0]):
        left = memory[h]
        for i in range(2):
            term = left.astype(jnp.bfloat16)
            terms[h, :, i * size : (i + 1) * size] = term
            left = left - term.astype(jnp.float32)


def update_memory(memory, key, write, retain, updated):
    heads, size = key.shape
    rest = jnp.zeros((size - heads, size), jnp.float32)
    turned = jnp.concatenate([key[...], rest], axis=0).T
    for h in range(heads):
        row = slice(h, h + 1)
        updated[h] = retain[row, :] * memory[h] + turned[:, row] * write[row, :]


def by_core(own, partner):
    first = place()[1] == 0
    low, high = jnp.where(first, own, partner), jnp.where(first, partner, own)
    return jnp.concatenate([low, high], axis=-1)


def chip_at(distance):
    chip, core = place()
    return chip ^ jnp.where(core == 0, distance[0], distance[1])


def mix_out(distances, tokens, partner_tokens, *refs):
    count = len(distances)
    got, (weight, partner_weight, block, middle, rows, wide) = refs[:count], refs[count:]
    for piece, distance in zip(got, distances):
        for c in range(2):
            rows[pl.ds(2 * chip_at(distance) + c, 1), :] = piece[c : c + 1, :]
    left = rows[...].astype(jnp.bfloat16)
    branch = by_core(dot(left, weight[...]), dot(left, partner_weight[...]))
    whole = branch + by_core(tokens[...].astype(jnp.float32), partner_tokens[...].astype(jnp.float32))
    block[...] = whole.astype(jnp.bfloat16)
    wide[...] = whole
    middle[...] = wide[:, span(place()[1], middle.shape[1])].astype(jnp.bfloat16)


def up_pieces(got, distances, gain, weight, parts):
    for piece, distance in zip(got, distances):
        size, there = piece.shape[1], chip_at(distance)
        wide = piece[...].astype(jnp.float32)
        ready = (wide * gain[:, span(there, size)]).astype(jnp.bfloat16)
        squares = jnp.sum(wide * wide, axis=1, keepdims=True)
        parts.append((dot(ready, weight[span(there, size), :]), squares))


def up_first(distances, *refs):
    count = len(distances)
    got, (gain, weight, total, squares) = refs[:count], refs[count:]
    parts = []
    up_pieces(got, distances, gain, weight, parts)
    total[...] = sum(part[0] for part in parts)
    squares[...] = jnp.broadcast_to(sum(part[1] for part in parts), squares.shape)


def up_rest(chips, distances, *refs):
    count = len(distances)
    got, rest = refs[:count], refs[count:]
    *before, gain, weight, down, hidden_ref, leaving = rest
    parts = [(a[...], b[:, :1]) for a, b in zip(before[::2], before[1::2])]
    up_pieces(got, distances, gain, weight, parts)
    scale = lax.rsqrt(sum(part[1] for part in parts) / gain.shape[1] + epsilon)
    raised = jnp.maximum(sum(part[0] for part in parts) * scale, 0.0)
    hidden = (raised * raised).astype(jnp.bfloat16)
    hidden_ref[...] = hidden
    size = leaving.shape[2]
    for d in range(chips):
        leaving[d] = dot(hidden, down[:, span(other_lane(d), size)]).astype(jnp.bfloat16)


def down_own(chips, hidden, down, staying):
    size = staying.shape[2]
    for d in range(chips):
        staying[d] = dot(hidden[...], down[:, span(mine_lane(d), size)])


def kernel_device(
    chips,
    tokens,
    memory,
    mix_gain,
    w_query,
    w_key,
    w_value,
    w_gate,
    w_beta,
    w_decay,
    decay_rate,
    decay_bias,
    head_gain,
    w_out,
    ffn_gain,
    w_up,
    w_down,
):
    f32, bf16 = jnp.float32, jnp.bfloat16
    rows, features = tokens.shape
    width = mix_gain.shape[0]
    heads = w_beta.shape[1]
    size = head_gain.shape[0]
    units = w_up.shape[1]
    part = w_query.shape[1]

    got = far([tokens] * chips, chips)[1:]
    partner = near(tokens)
    (tokens,) = call(keep_near, [(tokens.shape, bf16)], [tokens], work=8e9)
    others = near(jnp.stack(got))
    weights = [weight.T for weight in (w_query, w_key, w_value, w_gate)]
    gain_in = mix_gain.reshape(1, width)
    total, squares, lifted = call(
        functools.partial(project_first, chips),
        [((rows, 4 * part), f32), ((rows, 128), f32), ((rows, width), bf16)],
        [tokens, partner, *got, gain_in, *weights],
    )
    scale_in, lifted, *leaving = call(
        functools.partial(project_rest, chips),
        [((rows, 128), f32), ((rows, width), bf16)] + [((2, 4 * part), f32)] * chips,
        [others, total, squares, lifted, gain_in, *weights],
        [pltpu.VMEM((rows, 4 * part), f32)],
    )
    strength, retain, partner_strength, partner_retain = call(
        gates,
        [((heads, size), f32)] * 4,
        [lifted, scale_in, w_beta.T, w_decay.T]
        + [value.reshape(1, heads) for value in (decay_rate, decay_bias)],
    )
    mine = jnp.stack(far(leaving, chips))
    matrix = memory.reshape(heads, size, size)
    shape = ((heads, size, 2 * size), bf16)
    (terms,) = call(split_memory, [shape], [matrix], work=5e8)
    (partner_terms,) = call(split_memory, [shape], [near(matrix)], work=5e8)
    mixed, key, write = call(
        functools.partial(read_memory, chips),
        [((2, heads * size), f32), ((heads, size), f32), ((heads, size), f32)],
        [mine, near(mine), strength, retain, terms, partner_strength, partner_retain, partner_terms]
        + [head_gain.reshape(1, size)],
        [pltpu.VMEM((2, 4, heads, size), f32)],
    )
    (updated,) = call(
        update_memory, [((heads, size, size), f32)], [matrix, key, write, retain], work=5e8
    )

    here = (0, 0)
    direct, passed = shared(mixed, chips)
    got, distances = zip((mixed, here), *direct, *passed)
    block, middle = call(
        functools.partial(mix_out, distances),
        [((rows, 2 * features), bf16), ((rows, features), bf16)],
        [tokens, partner, *got, w_out, near(w_out)],
        [pltpu.VMEM((rows, heads * size), f32), pltpu.VMEM((rows, 2 * features), f32)],
    )

    direct, passed = shared(block, chips)
    gain_mid = ffn_gain.reshape(1, width)
    sums = [((rows, units), f32), ((rows, 128), f32)]
    early = []
    for piece, distance in [(block, here), *direct[:-1]]:
        early += call(functools.partial(up_first, [distance]), sums, [piece, gain_mid, w_up])
    got, distances = zip(direct[-1], *passed)
    hidden, leaving = call(
        functools.partial(up_rest, chips, distances),
        [((rows, units), bf16), ((chips, rows, features), bf16)],
        [*got, *early, gain_mid, w_up, w_down],
    )
    arrived = near(leaving)
    (staying,) = call(
        functools.partial(down_own, chips), [((chips, rows, features), f32)], [hidden, w_down]
    )
    sums = staying + arrived.astype(f32)
    terms = far([sums[0]] + [sums[d].astype(bf16) for d in range(1, chips)], chips)
    down = sum(term.astype(f32) for term in terms)
    layer_out = (middle.astype(f32) + down).astype(bf16)
    return (layer_out, updated.reshape(memory.shape))


def per_device(chips, *arrays):
    tokens, memory, head_gain = arrays[0], arrays[1], arrays[11]
    fits = (
        memory.shape[0] == 1
        and tokens.shape[0] == 2 * chips
        and tokens.shape[1] % 128 == 0
        and arrays[3].shape[1] % 16 == 0
        and 2 * arrays[3].shape[1] % head_gain.shape[0] == 0
        and head_gain.shape[0] == 128
        and memory.shape[1] <= 128
    )
    return (kernel_device if fits else plain_device)(chips, *arrays)


def solution(mesh):
    chips = mesh.shape["kv"]
    placed = (
        P(("grp", "dp"), ("kv", "tp")),
        P(("grp", "dp", "kv", "tp"), None, None),
        P(),
        P(None, ("kv", "tp")),
        P(None, ("kv", "tp")),
        P(None, ("kv", "tp")),
        P(None, ("kv", "tp")),
        P(),
        P(),
        P(),
        P(),
        P(),
        P(None, ("kv", "tp")),
        P(),
        P(None, ("kv", "tp")),
        P(("kv", "tp"), None),
    )

    def step(*arrays):
        return per_device(chips, *arrays)

    return jax.shard_map(
        step,
        mesh=mesh,
        in_specs=placed,
        out_specs=(P(("grp", "dp"), ("kv", "tp")), P(("grp", "dp", "kv", "tp"), None, None)),
        check_vma=False,
    )
```

```python
import functools

import jax
import jax.numpy as jnp
from jax import lax
from jax.experimental import pallas as pl
from jax.experimental.pallas import tpu as pltpu
from jax.sharding import PartitionSpec as P


epsilon = 1e-06
axes = ("kv", "tp")


def by_distance(stack, chip):
    count = stack.shape[0]
    rest = stack.shape[1:]
    bit = 1
    while bit < count:
        split = stack.reshape((count // (2 * bit), 2, bit) + rest)
        flipped = jnp.where((chip & bit) != 0, split[:, ::-1], split)
        stack = flipped.reshape((count,) + rest)
        bit *= 2
    return stack


def far(pieces, chips):
    got = [pieces[0]]
    for d in range(1, chips):
        pairs = [(i, i ^ (2 * d + 1)) for i in range(2 * chips)]
        got.append(lax.ppermute(pieces[d], axes, pairs))
    return got


def shared(piece, chips):
    falling = list(range(chips - 1, 0, -1))
    direct, passed = [], []
    for at in range(0, len(falling), 2):
        far_one, less = falling[at], falling[min(at + 1, len(falling) - 1)]
        pairs = [(i, i ^ (2 * (far_one if i % 2 else less))) for i in range(2 * chips)]
        got = lax.ppermute(piece, axes, pairs)
        direct.append((got, (less, far_one)))
        if less != far_one:
            passed.append((near(got), (far_one, less)))
    return direct, passed


def near(value):
    return lax.ppermute(value, "tp", [(0, 1), (1, 0)])


def merge(mine, other, chip, core):
    count = mine.shape[0]
    own = (jnp.arange(count) == 0).reshape((count,) + (1,) * (mine.ndim - 1))
    low_is_mine = own == (core == 0)
    low = jnp.where(low_is_mine, mine, other)
    high = jnp.where(low_is_mine, other, mine)
    both = by_distance(jnp.stack([low, high], axis=1), chip)
    return both.reshape((2 * count,) + mine.shape[1:])


def gather(piece, chips, chip, core):
    mine = jnp.stack(far([piece] * chips, chips))
    return merge(mine, near(mine), chip, core)


def gather_features(piece, chips, chip, core):
    parts = gather(piece, chips, chip, core)
    return jnp.concatenate([parts[i] for i in range(2 * chips)], axis=1)


def delta_step(queries, keys_in, values, gates, strength, log_decay, memory, head_gain):
    count = queries.shape[0]
    heads = strength.shape[1]
    size = head_gain.shape[0]
    highest = lax.Precision.HIGHEST
    query_wide = queries.astype(jnp.float32).reshape(count, heads, size)
    key_wide = keys_in.astype(jnp.float32).reshape(count, heads, size)
    value_wide = values.astype(jnp.float32).reshape(count, heads, size)
    gate_wide = gates.astype(jnp.float32).reshape(count, heads, size)
    unit_key = key_wide * lax.rsqrt(jnp.sum(key_wide * key_wide, axis=-1, keepdims=True) + epsilon)
    matrix = memory.reshape(count, heads, size, size)
    recall = jnp.einsum("bhk,bhkv->bhv", unit_key, matrix, precision=highest)
    retain = jnp.exp(log_decay)[:, :, None, None]
    scaled = strength[:, :, None]
    erased = matrix - jnp.einsum("bhk,bhv->bhkv", unit_key, scaled * recall, precision=highest)
    written = jnp.einsum("bhk,bhv->bhkv", unit_key, scaled * value_wide, precision=highest)
    updated = retain * erased + written
    readout = jnp.einsum("bhk,bhkv->bhv", query_wide, updated, precision=highest)
    normed = readout * lax.rsqrt(jnp.mean(readout * readout, axis=-1, keepdims=True) + epsilon)
    normed = normed * head_gain * jax.nn.silu(gate_wide)
    return (
        updated.reshape(count, heads, size * size),
        normed.reshape(count, heads * size).astype(jnp.bfloat16),
    )


def plain_device(
    chips,
    tokens,
    memory,
    mix_gain,
    w_query,
    w_key,
    w_value,
    w_gate,
    w_beta,
    w_decay,
    decay_rate,
    decay_bias,
    head_gain,
    w_out,
    ffn_gain,
    w_up,
    w_down,
):
    rows = tokens.shape[0]
    owned = memory.shape[0]
    width = mix_gain.shape[0]
    chip = lax.axis_index("kv")
    core = lax.axis_index("tp")
    own_start = lax.axis_index(axes) * owned
    wide = tokens.astype(jnp.float32)

    def lifted_of(whole, gain):
        whole_wide = whole.astype(jnp.float32)
        scale = lax.rsqrt(jnp.sum(whole_wide * whole_wide, axis=1) / width + epsilon)
        return (whole_wide * gain).astype(jnp.bfloat16), scale[:, None]

    def project(value, weight):
        return jnp.dot(value, weight, preferred_element_type=jnp.float32)

    lifted_in, scale_in = lifted_of(gather_features(tokens, chips, chip, core), mix_gain)
    sent = jnp.stack(
        [
            (project(lifted_in, weight) * scale_in).astype(jnp.bfloat16)
            for weight in (w_query, w_key, w_value, w_gate)
        ],
        axis=1,
    )
    strength_all = jax.nn.sigmoid(project(lifted_in, w_beta) * scale_in)
    decay_all = -decay_rate * jax.nn.softplus(project(lifted_in, w_decay) * scale_in + decay_bias)
    strength = lax.dynamic_slice_in_dim(strength_all, own_start, owned, 0)
    log_decay = lax.dynamic_slice_in_dim(decay_all, own_start, owned, 0)

    part = sent.shape[2]
    leaving = by_distance(sent.reshape(chips, 2, owned, 4, part), chip)
    mine = jnp.stack(far([leaving[d] for d in range(chips)], chips))
    other = near(mine)
    pick = lambda both: jnp.where(core == 0, both[:, 0], both[:, 1])
    whole = merge(pick(mine), pick(other), chip, core)
    whole = jnp.transpose(whole, (2, 1, 0, 3)).reshape(4, owned, 2 * chips * part)
    updated, mixed = delta_step(
        whole[0], whole[1], whole[2], whole[3], strength, log_decay, memory, head_gain
    )

    mixed_all = gather(mixed, chips, chip, core).reshape(rows, mixed.shape[1])
    middle = (wide + project(mixed_all, w_out)).astype(jnp.bfloat16)
    middle_wide = middle.astype(jnp.float32)
    lifted_mid, scale_mid = lifted_of(gather_features(middle, chips, chip, core), ffn_gain)
    raised = project(lifted_mid, w_up)
    hidden = jnp.square(jax.nn.relu(raised * scale_mid)).astype(jnp.bfloat16)
    terms = project(hidden, w_down).astype(jnp.bfloat16)

    features = tokens.shape[1]
    blocks = jnp.stack([terms[:, i * 2 * features : (i + 1) * 2 * features] for i in range(chips)])
    leaving = by_distance(blocks, chip)
    total = sum(
        (got.astype(jnp.float32) for got in far([leaving[d] for d in range(chips)], chips))
    )
    low, high = total[:, :features], total[:, features:]
    arrived = near(jnp.where(core == 0, high, low))
    down = jnp.where(core == 0, low, high) + arrived
    layer_out = (middle_wide + down).astype(jnp.bfloat16)
    return (layer_out, updated)


def place():
    return lax.axis_index("kv"), lax.axis_index("tp")


def mine_lane(d):
    chip, core = place()
    return 2 * (chip ^ d) + (core if d == 0 else 1 - core)


def other_lane(d):
    chip, core = place()
    return 2 * (chip ^ d) + (1 - core if d == 0 else core)


def span(lane, size):
    return pl.ds(pl.multiple_of(lane * size, size), size)


def dot_rows(left, right):
    return lax.dot_general(left, right, (((1,), (1,)), ((), ())), preferred_element_type=jnp.float32)


def dot(left, right):
    return jnp.dot(left, right, preferred_element_type=jnp.float32)


def call(body, outs, args, scratch=(), work=1e9):
    vmem = pl.BlockSpec(memory_space=pltpu.VMEM)
    return pl.pallas_call(
        body,
        out_shape=[jax.ShapeDtypeStruct(shape, kind) for shape, kind in outs],
        in_specs=[vmem] * len(args),
        out_specs=[vmem] * len(outs),
        scratch_shapes=list(scratch),
        compiler_params=pltpu.CompilerParams(vmem_limit_bytes=16 << 20),
        cost_estimate=pl.CostEstimate(flops=int(work), bytes_accessed=0, transcendentals=0),
    )(*args)


def keep_near(tokens, near_ref):
    near_ref[...] = tokens[...]


def project_piece(piece, lane, gain, weights, lifted, parts):
    size = piece.shape[1]
    wide = piece.astype(jnp.float32)
    ready = (wide * gain[:, span(lane, size)]).astype(jnp.bfloat16)
    lifted[:, span(lane, size)] = ready
    stacked = jnp.concatenate([weight[:, span(lane, size)] for weight in weights], axis=0)
    parts.append((dot_rows(ready, stacked), jnp.sum(wide * wide, axis=1, keepdims=True)))


def project_first(chips, tokens, partner, *refs):
    got, (gain, *rest) = refs[: chips - 1], refs[chips - 1 :]
    weights, (total, squares, lifted) = rest[:4], rest[4:]
    lifted[...] = jnp.zeros_like(lifted)
    parts = []
    project_piece(tokens[...], mine_lane(0), gain, weights, lifted, parts)
    project_piece(partner[...], other_lane(0), gain, weights, lifted, parts)
    for d in range(1, chips):
        project_piece(got[d - 1][...], mine_lane(d), gain, weights, lifted, parts)
    total[...] = sum(part[0] for part in parts)
    squares[...] = jnp.broadcast_to(sum(part[1] for part in parts), squares.shape)


def project_rest(chips, others, before, before_squares, before_lifted, gain, *rest):
    weights, (scale_ref, lifted, early, farthest), sent = rest[:4], rest[4:-1], rest[-1]
    lifted[...] = before_lifted[...]
    parts = [(before[...], before_squares[:, :1])]
    for d in range(1, chips):
        project_piece(others[d - 1], other_lane(d), gain, weights, lifted, parts)
    squares = sum(part[1] for part in parts)
    scale = lax.rsqrt(squares / lifted.shape[1] + epsilon)
    total = sum(part[0] for part in parts) * scale
    sent[...] = total.astype(jnp.bfloat16).astype(jnp.float32)
    scale_ref[...] = jnp.broadcast_to(scale, scale_ref.shape)
    chip, _ = place()
    for d in range(chips):
        for c in range(2):
            row = sent[pl.ds(2 * (chip ^ d) + c, 1), :]
            if d < chips - 1:
                early[d, c : c + 1, :] = row
            else:
                farthest[c : c + 1, :] = row


def column(row, heads):
    there = lax.broadcasted_iota(jnp.int32, (heads, heads), 0)
    here = lax.broadcasted_iota(jnp.int32, (heads, heads), 1)
    return jnp.sum(jnp.where(there == here, row, 0.0), axis=1, keepdims=True)


def gates(lifted, scale, w_beta, w_decay, rate, bias, *outs):
    heads = w_beta.shape[0]
    beta_all, decay_all = dot_rows(w_beta[...], lifted[...]), dot_rows(w_decay[...], lifted[...])
    bias_column, rate_column = column(bias[...], heads), column(rate[...], heads)
    for lane, (strength, retain) in ((mine_lane(0), outs[:2]), (other_lane(0), outs[2:])):
        scale_own = scale[pl.ds(lane, 1), :][:, :1]
        here = lax.broadcasted_iota(jnp.int32, beta_all.shape, 1) == lane

        def own(every):
            return jnp.sum(jnp.where(here, every, 0.0), axis=1, keepdims=True) * scale_own

        value = own(decay_all) + bias_column
        soft = jnp.maximum(value, 0.0) + jnp.log1p(jnp.exp(-jnp.abs(value)))
        decay = jnp.exp(-rate_column * soft)
        beta = 1.0 / (1.0 + jnp.exp(-own(beta_all)))
        strength[...] = jnp.broadcast_to(beta, strength.shape)
        retain[...] = jnp.broadcast_to(decay, retain.shape)


def read_row(chips, row, mine, other, strength, retain, terms, head_gain, parts):
    heads, size = strength.shape
    chip, core = place()
    part = mine.shape[2] // 4
    across = 2 * part // size
    for there in range(chips):
        d = chip ^ there
        own = mine[d, pl.ds(row, 1), :]
        partner = other[d, pl.ds(row, 1), :]
        straight = (d == 0) == (core == 0)
        low = jnp.where(straight, own, partner)
        high = jnp.where(straight, partner, own)
        for t in range(4):
            cut = slice(t * part, (t + 1) * part)
            pair = jnp.concatenate([low[:, cut], high[:, cut]], axis=1)
            for i in range(across):
                h = there * across + i
                parts[t, h : h + 1, :] = pair[:, i * size : (i + 1) * size]
    query, key, value, gate = parts[0], parts[1], parts[2], parts[3]
    shrink = lax.rsqrt(jnp.sum(key * key, axis=1, keepdims=True) + epsilon)
    padded = -(-heads // 16) * 16
    pad = [jnp.zeros((padded - heads, size), jnp.float32)] if padded > heads else []
    left = jnp.concatenate([key, *pad, query, *pad], axis=0).astype(jnp.bfloat16)
    at = lax.rem(lax.broadcasted_iota(jnp.int32, (2 * padded, 2 * size), 0), padded)
    found = sum(jnp.where(at == h, dot(left, terms[h]), 0.0) for h in range(heads))
    found = found[:, :size] + found[:, size:]
    recall, read = found[:heads] * shrink, found[padded : padded + heads]
    write = shrink * strength[...] * (value - retain[...] * recall)
    readout = retain[...] * read + jnp.sum(key * query, axis=1, keepdims=True) * write
    normed = readout * lax.rsqrt(jnp.mean(readout * readout, axis=1, keepdims=True) + epsilon)
    normed = normed * head_gain[...] * (gate / (1.0 + jnp.exp(-gate)))
    return normed.astype(jnp.bfloat16).astype(jnp.float32), key, write


def read_memory(chips, mine, other, *refs):
    outer, (head_gain, mixed, key_ref, write_ref, parts) = refs[:6], refs[6:]
    heads, size = key_ref.shape
    _, core = place()
    given = ((core, outer[0:3]), (1 - core, outer[3:6]))
    rows = [
        read_row(chips, row, mine, other, *three, head_gain, parts.at[i])
        for i, (row, three) in enumerate(given)
    ]
    own, partner = rows[0][0], rows[1][0]
    ordered = jnp.where(core == 0, own, partner), jnp.where(core == 0, partner, own)
    for h in range(heads):
        for c in range(2):
            mixed[c : c + 1, h * size : (h + 1) * size] = ordered[c][h : h + 1]
    key_ref[...] = rows[0][1]
    write_ref[...] = rows[0][2]


def split_memory(memory, terms):
    size = memory.shape[2]
    for h in range(memory.shape[0]):
        left = memory[h]
        for i in range(2):
            term = left.astype(jnp.bfloat16)
            terms[h, :, i * size : (i + 1) * size] = term
            left = left - term.astype(jnp.float32)


def update_memory(memory, key, write, retain, updated):
    heads, size = key.shape
    rest = jnp.zeros((size - heads, size), jnp.float32)
    turned = jnp.concatenate([key[...], rest], axis=0).T
    for h in range(heads):
        row = slice(h, h + 1)
        updated[h] = retain[row, :] * memory[h] + turned[:, row] * write[row, :]


def by_core(own, partner):
    first = place()[1] == 0
    low, high = jnp.where(first, own, partner), jnp.where(first, partner, own)
    return jnp.concatenate([low, high], axis=-1)


def chip_at(distance):
    chip, core = place()
    return chip ^ jnp.where(core == 0, distance[0], distance[1])


def mix_out(distances, tokens, partner_tokens, *refs):
    count = len(distances)
    got, (weight, partner_weight, block, middle, rows, wide) = refs[:count], refs[count:]
    for piece, distance in zip(got, distances):
        for c in range(2):
            rows[pl.ds(2 * chip_at(distance) + c, 1), :] = piece[c : c + 1, :]
    left = rows[...].astype(jnp.bfloat16)
    branch = by_core(dot(left, weight[...]), dot(left, partner_weight[...]))
    whole = branch + by_core(tokens[...].astype(jnp.float32), partner_tokens[...].astype(jnp.float32))
    block[...] = whole.astype(jnp.bfloat16)
    wide[...] = whole
    middle[...] = wide[:, span(place()[1], middle.shape[1])].astype(jnp.bfloat16)


def up_pieces(got, distances, gain, weight, parts):
    for piece, distance in zip(got, distances):
        size, there = piece.shape[1], chip_at(distance)
        wide = piece[...].astype(jnp.float32)
        ready = (wide * gain[:, span(there, size)]).astype(jnp.bfloat16)
        squares = jnp.sum(wide * wide, axis=1, keepdims=True)
        parts.append((dot(ready, weight[span(there, size), :]), squares))


def up_first(distances, *refs):
    count = len(distances)
    got, (gain, weight, total, squares) = refs[:count], refs[count:]
    parts = []
    up_pieces(got, distances, gain, weight, parts)
    total[...] = sum(part[0] for part in parts)
    squares[...] = jnp.broadcast_to(sum(part[1] for part in parts), squares.shape)


def up_rest(chips, distances, *refs):
    count = len(distances)
    got, rest = refs[:count], refs[count:]
    *before, gain, weight, down, hidden_ref, leaving, farthest = rest
    parts = [(a[...], b[:, :1]) for a, b in zip(before[::2], before[1::2])]
    up_pieces(got, distances, gain, weight, parts)
    scale = lax.rsqrt(sum(part[1] for part in parts) / gain.shape[1] + epsilon)
    raised = jnp.maximum(sum(part[0] for part in parts) * scale, 0.0)
    hidden = (raised * raised).astype(jnp.bfloat16)
    hidden_ref[...] = hidden
    size = leaving.shape[2]
    for d in range(chips - 1):
        leaving[d] = dot(hidden, down[:, span(other_lane(d), size)]).astype(jnp.bfloat16)
    across = span(place()[0] ^ (chips - 1), 2 * size)
    farthest[...] = dot(hidden, down[:, across]).astype(jnp.bfloat16)


def down_own(chips, hidden, down, staying):
    size = staying.shape[2]
    for d in range(chips - 1):
        staying[d] = dot(hidden[...], down[:, span(mine_lane(d), size)])


def add_up(middle, own, farthest, passed, *refs):
    *got, out = refs
    half = span(place()[1], out.shape[1])
    total = own[...]
    for piece in (farthest[:, half], passed[:, half], *(piece[...] for piece in got)):
        total = total + piece.astype(jnp.float32)
    out[...] = (middle[...].astype(jnp.float32) + total).astype(jnp.bfloat16)


def kernel_device(
    chips,
    tokens,
    memory,
    mix_gain,
    w_query,
    w_key,
    w_value,
    w_gate,
    w_beta,
    w_decay,
    decay_rate,
    decay_bias,
    head_gain,
    w_out,
    ffn_gain,
    w_up,
    w_down,
):
    f32, bf16 = jnp.float32, jnp.bfloat16
    rows, features = tokens.shape
    width = mix_gain.shape[0]
    heads = w_beta.shape[1]
    size = head_gain.shape[0]
    units = w_up.shape[1]
    part = w_query.shape[1]

    got = far([tokens] * chips, chips)[1:]
    partner = near(tokens)
    (tokens,) = call(keep_near, [(tokens.shape, bf16)], [tokens], work=8e9)
    others = near(jnp.stack(got))
    weights = [weight.T for weight in (w_query, w_key, w_value, w_gate)]
    gain_in = mix_gain.reshape(1, width)
    total, squares, lifted = call(
        functools.partial(project_first, chips),
        [((rows, 4 * part), f32), ((rows, 128), f32), ((rows, width), bf16)],
        [tokens, partner, *got, gain_in, *weights],
    )
    scale_in, lifted, early, farthest = call(
        functools.partial(project_rest, chips),
        [((rows, 128), f32), ((rows, width), bf16)]
        + [((chips - 1, 2, 4 * part), f32), ((2, 4 * part), f32)],
        [others, total, squares, lifted, gain_in, *weights],
        [pltpu.VMEM((rows, 4 * part), f32)],
    )
    strength, retain, partner_strength, partner_retain = call(
        gates,
        [((heads, size), f32)] * 4,
        [lifted, scale_in, w_beta.T, w_decay.T]
        + [value.reshape(1, heads) for value in (decay_rate, decay_bias)],
    )
    passed = near(early)
    both = [jnp.stack([early[d], passed[d]]) for d in range(chips - 1)]
    got = far(both + [farthest], chips)
    mine = jnp.stack([piece[0] for piece in got[:-1]] + [got[-1]])
    other = jnp.stack([piece[1] for piece in got[:-1]] + [near(got[-1])])
    matrix = memory.reshape(heads, size, size)
    shape = ((heads, size, 2 * size), bf16)
    (terms,) = call(split_memory, [shape], [matrix], work=5e8)
    moved = near(matrix)
    (partner_terms,) = call(split_memory, [shape], [moved], work=5e8)
    mixed, key, write = call(
        functools.partial(read_memory, chips),
        [((2, heads * size), f32), ((heads, size), f32), ((heads, size), f32)],
        [mine, other, strength, retain, terms, partner_strength, partner_retain, partner_terms]
        + [head_gain.reshape(1, size)],
        [pltpu.VMEM((2, 4, heads, size), f32)],
    )
    (updated,) = call(
        update_memory, [((heads, size, size), f32)], [matrix, key, write, retain], work=5e8
    )

    here = (0, 0)
    direct, passed = shared(mixed, chips)
    got, distances = zip((mixed, here), *direct, *passed)
    block, middle = call(
        functools.partial(mix_out, distances),
        [((rows, 2 * features), bf16), ((rows, features), bf16)],
        [tokens, partner, *got, w_out, near(w_out)],
        [pltpu.VMEM((rows, heads * size), f32), pltpu.VMEM((rows, 2 * features), f32)],
    )

    direct, passed = shared(block, chips)
    gain_mid = ffn_gain.reshape(1, width)
    sums = [((rows, units), f32), ((rows, 128), f32)]
    early = []
    for piece, distance in [(block, here), *direct[:-1]]:
        early += call(functools.partial(up_first, [distance]), sums, [piece, gain_mid, w_up])
    got, distances = zip(direct[-1], *passed)
    hidden, leaving, farthest = call(
        functools.partial(up_rest, chips, distances),
        [((rows, units), bf16), ((chips - 1, rows, features), bf16), ((rows, 2 * features), bf16)],
        [*got, *early, gain_mid, w_up, w_down],
    )
    arrived = near(leaving)
    (staying,) = call(
        functools.partial(down_own, chips),
        [((chips - 1, rows, features), f32)],
        [hidden, w_down],
    )
    sums = staying + arrived.astype(f32)
    terms = [sums[d].astype(bf16) for d in range(chips - 1)] + [farthest]
    *got, farthest = far(terms, chips)[1:]
    (layer_out,) = call(
        add_up,
        [((rows, features), bf16)],
        [middle, sums[0], farthest, near(farthest), *got],
    )
    return (layer_out, updated.reshape(memory.shape))


def per_device(chips, *arrays):
    tokens, memory, head_gain = arrays[0], arrays[1], arrays[11]
    fits = (
        memory.shape[0] == 1
        and tokens.shape[0] == 2 * chips
        and tokens.shape[1] % 128 == 0
        and arrays[3].shape[1] % 16 == 0
        and 2 * arrays[3].shape[1] % head_gain.shape[0] == 0
        and head_gain.shape[0] == 128
        and memory.shape[1] <= 128
    )
    return (kernel_device if fits else plain_device)(chips, *arrays)


def solution(mesh):
    chips = mesh.shape["kv"]
    placed = (
        P(("grp", "dp"), ("kv", "tp")),
        P(("grp", "dp", "kv", "tp"), None, None),
        P(),
        P(None, ("kv", "tp")),
        P(None, ("kv", "tp")),
        P(None, ("kv", "tp")),
        P(None, ("kv", "tp")),
        P(),
        P(),
        P(),
        P(),
        P(),
        P(None, ("kv", "tp")),
        P(),
        P(None, ("kv", "tp")),
        P(("kv", "tp"), None),
    )

    def step(*arrays):
        return per_device(chips, *arrays)

    return jax.shard_map(
        step,
        mesh=mesh,
        in_specs=placed,
        out_specs=(P(("grp", "dp"), ("kv", "tp")), P(("grp", "dp", "kv", "tp"), None, None)),
        check_vma=False,
    )
```

```python
import functools

import jax
import jax.numpy as jnp
from jax import lax
from jax.experimental import pallas as pl
from jax.experimental.pallas import tpu as pltpu
from jax.sharding import PartitionSpec as P


epsilon = 1e-06
axes = ("kv", "tp")


def by_distance(stack, chip):
    count = stack.shape[0]
    rest = stack.shape[1:]
    bit = 1
    while bit < count:
        split = stack.reshape((count // (2 * bit), 2, bit) + rest)
        flipped = jnp.where((chip & bit) != 0, split[:, ::-1], split)
        stack = flipped.reshape((count,) + rest)
        bit *= 2
    return stack


def far(pieces, chips):
    got = [pieces[0]]
    for d in range(1, chips):
        pairs = [(i, i ^ (2 * d + 1)) for i in range(2 * chips)]
        got.append(lax.ppermute(pieces[d], axes, pairs))
    return got


def shared(piece, chips):
    falling = list(range(chips - 1, 0, -1))
    direct, passed = [], []
    for at in range(0, len(falling), 2):
        far_one, less = falling[at], falling[min(at + 1, len(falling) - 1)]
        pairs = [(i, i ^ (2 * (far_one if i % 2 else less))) for i in range(2 * chips)]
        got = lax.ppermute(piece, axes, pairs)
        direct.append((got, (less, far_one)))
        if less != far_one:
            passed.append((near(got), (far_one, less)))
    return direct, passed


def near(value):
    return lax.ppermute(value, "tp", [(0, 1), (1, 0)])


def merge(mine, other, chip, core):
    count = mine.shape[0]
    own = (jnp.arange(count) == 0).reshape((count,) + (1,) * (mine.ndim - 1))
    low_is_mine = own == (core == 0)
    low = jnp.where(low_is_mine, mine, other)
    high = jnp.where(low_is_mine, other, mine)
    both = by_distance(jnp.stack([low, high], axis=1), chip)
    return both.reshape((2 * count,) + mine.shape[1:])


def gather(piece, chips, chip, core):
    mine = jnp.stack(far([piece] * chips, chips))
    return merge(mine, near(mine), chip, core)


def gather_features(piece, chips, chip, core):
    parts = gather(piece, chips, chip, core)
    return jnp.concatenate([parts[i] for i in range(2 * chips)], axis=1)


def delta_step(queries, keys_in, values, gates, strength, log_decay, memory, head_gain):
    count = queries.shape[0]
    heads = strength.shape[1]
    size = head_gain.shape[0]
    highest = lax.Precision.HIGHEST
    query_wide = queries.astype(jnp.float32).reshape(count, heads, size)
    key_wide = keys_in.astype(jnp.float32).reshape(count, heads, size)
    value_wide = values.astype(jnp.float32).reshape(count, heads, size)
    gate_wide = gates.astype(jnp.float32).reshape(count, heads, size)
    unit_key = key_wide * lax.rsqrt(jnp.sum(key_wide * key_wide, axis=-1, keepdims=True) + epsilon)
    matrix = memory.reshape(count, heads, size, size)
    recall = jnp.einsum("bhk,bhkv->bhv", unit_key, matrix, precision=highest)
    retain = jnp.exp(log_decay)[:, :, None, None]
    scaled = strength[:, :, None]
    erased = matrix - jnp.einsum("bhk,bhv->bhkv", unit_key, scaled * recall, precision=highest)
    written = jnp.einsum("bhk,bhv->bhkv", unit_key, scaled * value_wide, precision=highest)
    updated = retain * erased + written
    readout = jnp.einsum("bhk,bhkv->bhv", query_wide, updated, precision=highest)
    normed = readout * lax.rsqrt(jnp.mean(readout * readout, axis=-1, keepdims=True) + epsilon)
    normed = normed * head_gain * jax.nn.silu(gate_wide)
    return (
        updated.reshape(count, heads, size * size),
        normed.reshape(count, heads * size).astype(jnp.bfloat16),
    )


def plain_device(
    chips,
    tokens,
    memory,
    mix_gain,
    w_query,
    w_key,
    w_value,
    w_gate,
    w_beta,
    w_decay,
    decay_rate,
    decay_bias,
    head_gain,
    w_out,
    ffn_gain,
    w_up,
    w_down,
):
    rows = tokens.shape[0]
    owned = memory.shape[0]
    width = mix_gain.shape[0]
    chip = lax.axis_index("kv")
    core = lax.axis_index("tp")
    own_start = lax.axis_index(axes) * owned
    wide = tokens.astype(jnp.float32)

    def lifted_of(whole, gain):
        whole_wide = whole.astype(jnp.float32)
        scale = lax.rsqrt(jnp.sum(whole_wide * whole_wide, axis=1) / width + epsilon)
        return (whole_wide * gain).astype(jnp.bfloat16), scale[:, None]

    def project(value, weight):
        return jnp.dot(value, weight, preferred_element_type=jnp.float32)

    lifted_in, scale_in = lifted_of(gather_features(tokens, chips, chip, core), mix_gain)
    sent = jnp.stack(
        [
            (project(lifted_in, weight) * scale_in).astype(jnp.bfloat16)
            for weight in (w_query, w_key, w_value, w_gate)
        ],
        axis=1,
    )
    strength_all = jax.nn.sigmoid(project(lifted_in, w_beta) * scale_in)
    decay_all = -decay_rate * jax.nn.softplus(project(lifted_in, w_decay) * scale_in + decay_bias)
    strength = lax.dynamic_slice_in_dim(strength_all, own_start, owned, 0)
    log_decay = lax.dynamic_slice_in_dim(decay_all, own_start, owned, 0)

    part = sent.shape[2]
    leaving = by_distance(sent.reshape(chips, 2, owned, 4, part), chip)
    mine = jnp.stack(far([leaving[d] for d in range(chips)], chips))
    other = near(mine)
    pick = lambda both: jnp.where(core == 0, both[:, 0], both[:, 1])
    whole = merge(pick(mine), pick(other), chip, core)
    whole = jnp.transpose(whole, (2, 1, 0, 3)).reshape(4, owned, 2 * chips * part)
    updated, mixed = delta_step(
        whole[0], whole[1], whole[2], whole[3], strength, log_decay, memory, head_gain
    )

    mixed_all = gather(mixed, chips, chip, core).reshape(rows, mixed.shape[1])
    middle = (wide + project(mixed_all, w_out)).astype(jnp.bfloat16)
    middle_wide = middle.astype(jnp.float32)
    lifted_mid, scale_mid = lifted_of(gather_features(middle, chips, chip, core), ffn_gain)
    raised = project(lifted_mid, w_up)
    hidden = jnp.square(jax.nn.relu(raised * scale_mid)).astype(jnp.bfloat16)
    terms = project(hidden, w_down).astype(jnp.bfloat16)

    features = tokens.shape[1]
    blocks = jnp.stack([terms[:, i * 2 * features : (i + 1) * 2 * features] for i in range(chips)])
    leaving = by_distance(blocks, chip)
    total = sum(
        (got.astype(jnp.float32) for got in far([leaving[d] for d in range(chips)], chips))
    )
    low, high = total[:, :features], total[:, features:]
    arrived = near(jnp.where(core == 0, high, low))
    down = jnp.where(core == 0, low, high) + arrived
    layer_out = (middle_wide + down).astype(jnp.bfloat16)
    return (layer_out, updated)


def place():
    return lax.axis_index("kv"), lax.axis_index("tp")


def mine_lane(d):
    chip, core = place()
    return 2 * (chip ^ d) + (core if d == 0 else 1 - core)


def other_lane(d):
    chip, core = place()
    return 2 * (chip ^ d) + (1 - core if d == 0 else core)


def span(lane, size):
    return pl.ds(pl.multiple_of(lane * size, size), size)


def dot_rows(left, right):
    return lax.dot_general(left, right, (((1,), (1,)), ((), ())), preferred_element_type=jnp.float32)


def dot(left, right):
    return jnp.dot(left, right, preferred_element_type=jnp.float32)


def call(body, outs, args, scratch=(), work=1e9):
    vmem = pl.BlockSpec(memory_space=pltpu.VMEM)
    return pl.pallas_call(
        body,
        out_shape=[jax.ShapeDtypeStruct(shape, kind) for shape, kind in outs],
        in_specs=[vmem] * len(args),
        out_specs=[vmem] * len(outs),
        scratch_shapes=list(scratch),
        compiler_params=pltpu.CompilerParams(vmem_limit_bytes=16 << 20),
        cost_estimate=pl.CostEstimate(flops=int(work), bytes_accessed=0, transcendentals=0),
    )(*args)


def keep_near(tokens, near_ref):
    near_ref[...] = tokens[...]


def project_piece(piece, lane, gain, weights, lifted, parts):
    size = piece.shape[1]
    wide = piece.astype(jnp.float32)
    ready = (wide * gain[:, span(lane, size)]).astype(jnp.bfloat16)
    lifted[:, span(lane, size)] = ready
    stacked = jnp.concatenate([weight[:, span(lane, size)] for weight in weights], axis=0)
    parts.append((dot_rows(ready, stacked), jnp.sum(wide * wide, axis=1, keepdims=True)))


def project_first(chips, tokens, partner, *refs):
    got, (gain, *rest) = refs[: chips - 1], refs[chips - 1 :]
    weights, (total, squares, lifted) = rest[:4], rest[4:]
    lifted[...] = jnp.zeros_like(lifted)
    parts = []
    project_piece(tokens[...], mine_lane(0), gain, weights, lifted, parts)
    project_piece(partner[...], other_lane(0), gain, weights, lifted, parts)
    for d in range(1, chips):
        project_piece(got[d - 1][...], mine_lane(d), gain, weights, lifted, parts)
    total[...] = sum(part[0] for part in parts)
    squares[...] = jnp.broadcast_to(sum(part[1] for part in parts), squares.shape)


def project_rest(chips, others, before, before_squares, before_lifted, gain, *rest):
    weights, (scale_ref, lifted, early, farthest), sent = rest[:4], rest[4:-1], rest[-1]
    lifted[...] = before_lifted[...]
    parts = [(before[...], before_squares[:, :1])]
    for d in range(1, chips):
        project_piece(others[d - 1], other_lane(d), gain, weights, lifted, parts)
    squares = sum(part[1] for part in parts)
    scale = lax.rsqrt(squares / lifted.shape[1] + epsilon)
    total = sum(part[0] for part in parts) * scale
    sent[...] = total.astype(jnp.bfloat16).astype(jnp.float32)
    scale_ref[...] = jnp.broadcast_to(scale, scale_ref.shape)
    chip, _ = place()
    for d in range(chips):
        for c in range(2):
            row = sent[pl.ds(2 * (chip ^ d) + c, 1), :]
            if d < chips - 1:
                early[d, c : c + 1, :] = row
            else:
                farthest[c : c + 1, :] = row


def column(row, heads):
    there = lax.broadcasted_iota(jnp.int32, (heads, heads), 0)
    here = lax.broadcasted_iota(jnp.int32, (heads, heads), 1)
    return jnp.sum(jnp.where(there == here, row, 0.0), axis=1, keepdims=True)


def gates(lifted, scale, w_beta, w_decay, rate, bias, *outs):
    heads = w_beta.shape[0]
    beta_all, decay_all = dot_rows(w_beta[...], lifted[...]), dot_rows(w_decay[...], lifted[...])
    bias_column, rate_column = column(bias[...], heads), column(rate[...], heads)
    for lane, (strength, retain) in ((mine_lane(0), outs[:2]), (other_lane(0), outs[2:])):
        scale_own = scale[pl.ds(lane, 1), :][:, :1]
        here = lax.broadcasted_iota(jnp.int32, beta_all.shape, 1) == lane

        def own(every):
            return jnp.sum(jnp.where(here, every, 0.0), axis=1, keepdims=True) * scale_own

        value = own(decay_all) + bias_column
        soft = jnp.maximum(value, 0.0) + jnp.log1p(jnp.exp(-jnp.abs(value)))
        decay = jnp.exp(-rate_column * soft)
        beta = 1.0 / (1.0 + jnp.exp(-own(beta_all)))
        strength[...] = jnp.broadcast_to(beta, strength.shape)
        retain[...] = jnp.broadcast_to(decay, retain.shape)


def read_row(chips, row, mine, other, strength, retain, terms, head_gain, parts):
    heads, size = strength.shape
    chip, core = place()
    part = mine.shape[2] // 4
    across = 2 * part // size
    for there in range(chips):
        d = chip ^ there
        own = mine[d, pl.ds(row, 1), :]
        partner = other[d, pl.ds(row, 1), :]
        straight = (d == 0) == (core == 0)
        low = jnp.where(straight, own, partner)
        high = jnp.where(straight, partner, own)
        for t in range(4):
            cut = slice(t * part, (t + 1) * part)
            pair = jnp.concatenate([low[:, cut], high[:, cut]], axis=1)
            for i in range(across):
                h = there * across + i
                parts[t, h : h + 1, :] = pair[:, i * size : (i + 1) * size]
    query, key, value, gate = parts[0], parts[1], parts[2], parts[3]
    shrink = lax.rsqrt(jnp.sum(key * key, axis=1, keepdims=True) + epsilon)
    padded = -(-heads // 16) * 16
    pad = [jnp.zeros((padded - heads, size), jnp.float32)] if padded > heads else []
    left = jnp.concatenate([key, *pad, query, *pad], axis=0).astype(jnp.bfloat16)
    at = lax.rem(lax.broadcasted_iota(jnp.int32, (2 * padded, 2 * size), 0), padded)
    found = sum(jnp.where(at == h, dot(left, terms[h]), 0.0) for h in range(heads))
    found = found[:, :size] + found[:, size:]
    recall, read = found[:heads] * shrink, found[padded : padded + heads]
    write = shrink * strength[...] * (value - retain[...] * recall)
    readout = retain[...] * read + jnp.sum(key * query, axis=1, keepdims=True) * write
    normed = readout * lax.rsqrt(jnp.mean(readout * readout, axis=1, keepdims=True) + epsilon)
    normed = normed * head_gain[...] * (gate / (1.0 + jnp.exp(-gate)))
    return normed.astype(jnp.bfloat16).astype(jnp.float32), key, write


def read_memory(chips, mine, other, *refs):
    outer, (head_gain, mixed, key_ref, write_ref, parts) = refs[:6], refs[6:]
    heads, size = key_ref.shape
    _, core = place()
    given = ((core, outer[0:3]), (1 - core, outer[3:6]))
    rows = [
        read_row(chips, row, mine, other, *three, head_gain, parts.at[i])
        for i, (row, three) in enumerate(given)
    ]
    own, partner = rows[0][0], rows[1][0]
    ordered = jnp.where(core == 0, own, partner), jnp.where(core == 0, partner, own)
    for h in range(heads):
        for c in range(2):
            mixed[c : c + 1, h * size : (h + 1) * size] = ordered[c][h : h + 1]
    key_ref[...] = rows[0][1]
    write_ref[...] = rows[0][2]


def split_memory(memory, terms):
    size = memory.shape[2]
    for h in range(memory.shape[0]):
        left = memory[h]
        for i in range(2):
            term = left.astype(jnp.bfloat16)
            terms[h, :, i * size : (i + 1) * size] = term
            left = left - term.astype(jnp.float32)


def update_memory(memory, key, write, retain, updated):
    heads, size = key.shape
    rest = jnp.zeros((size - heads, size), jnp.float32)
    turned = jnp.concatenate([key[...], rest], axis=0).T
    for h in range(heads):
        row = slice(h, h + 1)
        updated[h] = retain[row, :] * memory[h] + turned[:, row] * write[row, :]


def by_core(own, partner):
    first = place()[1] == 0
    low, high = jnp.where(first, own, partner), jnp.where(first, partner, own)
    return jnp.concatenate([low, high], axis=-1)


def chip_at(distance):
    chip, core = place()
    return chip ^ jnp.where(core == 0, distance[0], distance[1])


def mix_out(distances, tokens, partner_tokens, *refs):
    count = len(distances)
    got, (weight, partner_weight, block, middle, rows, wide) = refs[:count], refs[count:]
    for piece, distance in zip(got, distances):
        for c in range(2):
            rows[pl.ds(2 * chip_at(distance) + c, 1), :] = piece[c : c + 1, :]
    left = rows[...].astype(jnp.bfloat16)
    branch = by_core(dot(left, weight[...]), dot(left, partner_weight[...]))
    whole = branch + by_core(tokens[...].astype(jnp.float32), partner_tokens[...].astype(jnp.float32))
    block[...] = whole.astype(jnp.bfloat16)
    wide[...] = whole
    middle[...] = wide[:, span(place()[1], middle.shape[1])].astype(jnp.bfloat16)


def up_pieces(got, distances, gain, weight, parts):
    for piece, distance in zip(got, distances):
        size, there = piece.shape[1], chip_at(distance)
        wide = piece[...].astype(jnp.float32)
        ready = (wide * gain[:, span(there, size)]).astype(jnp.bfloat16)
        squares = jnp.sum(wide * wide, axis=1, keepdims=True)
        parts.append((dot(ready, weight[span(there, size), :]), squares))


def up_first(distances, *refs):
    count = len(distances)
    got, (gain, weight, total, squares) = refs[:count], refs[count:]
    parts = []
    up_pieces(got, distances, gain, weight, parts)
    total[...] = sum(part[0] for part in parts)
    squares[...] = jnp.broadcast_to(sum(part[1] for part in parts), squares.shape)


def up_rest(chips, distances, *refs):
    count = len(distances)
    got, rest = refs[:count], refs[count:]
    *before, gain, weight, down, hidden_ref, leaving, farthest = rest
    parts = [(a[...], b[:, :1]) for a, b in zip(before[::2], before[1::2])]
    up_pieces(got, distances, gain, weight, parts)
    scale = lax.rsqrt(sum(part[1] for part in parts) / gain.shape[1] + epsilon)
    raised = jnp.maximum(sum(part[0] for part in parts) * scale, 0.0)
    hidden = (raised * raised).astype(jnp.bfloat16)
    hidden_ref[...] = hidden
    size = leaving.shape[2]
    for d in range(chips - 1):
        leaving[d] = dot(hidden, down[:, span(other_lane(d), size)]).astype(jnp.bfloat16)
    across = span(place()[0] ^ (chips - 1), 2 * size)
    farthest[...] = dot(hidden, down[:, across]).astype(jnp.bfloat16)


def down_own(d, hidden, down, arrived, total):
    own = dot(hidden[...], down[:, span(mine_lane(d), total.shape[1])])
    total[...] = (own + arrived[d].astype(jnp.float32)).astype(total.dtype)


def add_up(middle, own, farthest, passed, *refs):
    *got, out = refs
    half = span(place()[1], out.shape[1])
    total = own[...]
    for piece in (farthest[:, half], passed[:, half], *(piece[...] for piece in got)):
        total = total + piece.astype(jnp.float32)
    out[...] = (middle[...].astype(jnp.float32) + total).astype(jnp.bfloat16)


def kernel_device(
    chips,
    tokens,
    memory,
    mix_gain,
    w_query,
    w_key,
    w_value,
    w_gate,
    w_beta,
    w_decay,
    decay_rate,
    decay_bias,
    head_gain,
    w_out,
    ffn_gain,
    w_up,
    w_down,
):
    f32, bf16 = jnp.float32, jnp.bfloat16
    rows, features = tokens.shape
    width = mix_gain.shape[0]
    heads = w_beta.shape[1]
    size = head_gain.shape[0]
    units = w_up.shape[1]
    part = w_query.shape[1]

    got = far([tokens] * chips, chips)[1:]
    partner = near(tokens)
    (tokens,) = call(keep_near, [(tokens.shape, bf16)], [tokens], work=8e9)
    others = near(jnp.stack(got))
    weights = [weight.T for weight in (w_query, w_key, w_value, w_gate)]
    gain_in = mix_gain.reshape(1, width)
    total, squares, lifted = call(
        functools.partial(project_first, chips),
        [((rows, 4 * part), f32), ((rows, 128), f32), ((rows, width), bf16)],
        [tokens, partner, *got, gain_in, *weights],
    )
    scale_in, lifted, early, farthest = call(
        functools.partial(project_rest, chips),
        [((rows, 128), f32), ((rows, width), bf16)]
        + [((chips - 1, 2, 4 * part), f32), ((2, 4 * part), f32)],
        [others, total, squares, lifted, gain_in, *weights],
        [pltpu.VMEM((rows, 4 * part), f32)],
    )
    strength, retain, partner_strength, partner_retain = call(
        gates,
        [((heads, size), f32)] * 4,
        [lifted, scale_in, w_beta.T, w_decay.T]
        + [value.reshape(1, heads) for value in (decay_rate, decay_bias)],
    )
    passed = near(early)
    both = [jnp.stack([early[d], passed[d]]) for d in range(chips - 1)]
    got = far(both + [farthest], chips)
    mine = jnp.stack([piece[0] for piece in got[:-1]] + [got[-1]])
    other = jnp.stack([piece[1] for piece in got[:-1]] + [near(got[-1])])
    matrix = memory.reshape(heads, size, size)
    shape = ((heads, size, 2 * size), bf16)
    (terms,) = call(split_memory, [shape], [matrix], work=5e8)
    moved = near(matrix)
    (partner_terms,) = call(split_memory, [shape], [moved], work=5e8)
    mixed, key, write = call(
        functools.partial(read_memory, chips),
        [((2, heads * size), f32), ((heads, size), f32), ((heads, size), f32)],
        [mine, other, strength, retain, terms, partner_strength, partner_retain, partner_terms]
        + [head_gain.reshape(1, size)],
        [pltpu.VMEM((2, 4, heads, size), f32)],
    )
    (updated,) = call(
        update_memory, [((heads, size, size), f32)], [matrix, key, write, retain], work=5e8
    )

    here = (0, 0)
    direct, passed = shared(mixed, chips)
    got, distances = zip((mixed, here), *direct, *passed)
    block, middle = call(
        functools.partial(mix_out, distances),
        [((rows, 2 * features), bf16), ((rows, features), bf16)],
        [tokens, partner, *got, w_out, near(w_out)],
        [pltpu.VMEM((rows, heads * size), f32), pltpu.VMEM((rows, 2 * features), f32)],
    )

    direct, passed = shared(block, chips)
    gain_mid = ffn_gain.reshape(1, width)
    sums = [((rows, units), f32), ((rows, 128), f32)]
    early = []
    for piece, distance in [(block, here), *direct[:-1]]:
        early += call(functools.partial(up_first, [distance]), sums, [piece, gain_mid, w_up])
    got, distances = zip(direct[-1], *passed)
    hidden, leaving, farthest = call(
        functools.partial(up_rest, chips, distances),
        [((rows, units), bf16), ((chips - 1, rows, features), bf16), ((rows, 2 * features), bf16)],
        [*got, *early, gain_mid, w_up, w_down],
    )
    arrived = near(leaving)
    terms = []
    for d in range(chips - 1):
        terms += call(
            functools.partial(down_own, d),
            [((rows, features), bf16 if d else f32)],
            [hidden, w_down, arrived],
        )
    own = terms[0]
    terms.append(farthest)
    *got, farthest = far(terms, chips)[1:]
    (layer_out,) = call(
        add_up,
        [((rows, features), bf16)],
        [middle, own, farthest, near(farthest), *got],
    )
    return (layer_out, updated.reshape(memory.shape))


def per_device(chips, *arrays):
    tokens, memory, head_gain = arrays[0], arrays[1], arrays[11]
    fits = (
        memory.shape[0] == 1
        and tokens.shape[0] == 2 * chips
        and tokens.shape[1] % 128 == 0
        and arrays[3].shape[1] % 16 == 0
        and 2 * arrays[3].shape[1] % head_gain.shape[0] == 0
        and head_gain.shape[0] == 128
        and memory.shape[1] <= 128
    )
    return (kernel_device if fits else plain_device)(chips, *arrays)


def solution(mesh):
    chips = mesh.shape["kv"]
    placed = (
        P(("grp", "dp"), ("kv", "tp")),
        P(("grp", "dp", "kv", "tp"), None, None),
        P(),
        P(None, ("kv", "tp")),
        P(None, ("kv", "tp")),
        P(None, ("kv", "tp")),
        P(None, ("kv", "tp")),
        P(),
        P(),
        P(),
        P(),
        P(),
        P(None, ("kv", "tp")),
        P(),
        P(None, ("kv", "tp")),
        P(("kv", "tp"), None),
    )

    def step(*arrays):
        return per_device(chips, *arrays)

    return jax.shard_map(
        step,
        mesh=mesh,
        in_specs=placed,
        out_specs=(P(("grp", "dp"), ("kv", "tp")), P(("grp", "dp", "kv", "tp"), None, None)),
        check_vma=False,
    )
```

```python
import functools

import jax
import jax.numpy as jnp
from jax import lax
from jax.experimental import pallas as pl
from jax.experimental.pallas import tpu as pltpu
from jax.sharding import PartitionSpec as P


epsilon = 1e-06
axes = ("kv", "tp")


def by_distance(stack, chip):
    count = stack.shape[0]
    rest = stack.shape[1:]
    bit = 1
    while bit < count:
        split = stack.reshape((count // (2 * bit), 2, bit) + rest)
        flipped = jnp.where((chip & bit) != 0, split[:, ::-1], split)
        stack = flipped.reshape((count,) + rest)
        bit *= 2
    return stack


def far(pieces, chips):
    got = [pieces[0]]
    for d in range(1, chips):
        pairs = [(i, i ^ (2 * d + 1)) for i in range(2 * chips)]
        got.append(lax.ppermute(pieces[d], axes, pairs))
    return got


def shared(piece, chips):
    falling = list(range(chips - 1, 0, -1))
    direct, passed = [], []
    for at in range(0, len(falling), 2):
        far_one, less = falling[at], falling[min(at + 1, len(falling) - 1)]
        pairs = [(i, i ^ (2 * (far_one if i % 2 else less))) for i in range(2 * chips)]
        got = lax.ppermute(piece, axes, pairs)
        direct.append((got, (less, far_one)))
        if less != far_one:
            passed.append((near(got), (far_one, less)))
    return direct, passed


def near(value):
    return lax.ppermute(value, "tp", [(0, 1), (1, 0)])


def merge(mine, other, chip, core):
    count = mine.shape[0]
    own = (jnp.arange(count) == 0).reshape((count,) + (1,) * (mine.ndim - 1))
    low_is_mine = own == (core == 0)
    low = jnp.where(low_is_mine, mine, other)
    high = jnp.where(low_is_mine, other, mine)
    both = by_distance(jnp.stack([low, high], axis=1), chip)
    return both.reshape((2 * count,) + mine.shape[1:])


def gather(piece, chips, chip, core):
    mine = jnp.stack(far([piece] * chips, chips))
    return merge(mine, near(mine), chip, core)


def gather_features(piece, chips, chip, core):
    parts = gather(piece, chips, chip, core)
    return jnp.concatenate([parts[i] for i in range(2 * chips)], axis=1)


def delta_step(queries, keys_in, values, gates, strength, log_decay, memory, head_gain):
    count = queries.shape[0]
    heads = strength.shape[1]
    size = head_gain.shape[0]
    highest = lax.Precision.HIGHEST
    query_wide = queries.astype(jnp.float32).reshape(count, heads, size)
    key_wide = keys_in.astype(jnp.float32).reshape(count, heads, size)
    value_wide = values.astype(jnp.float32).reshape(count, heads, size)
    gate_wide = gates.astype(jnp.float32).reshape(count, heads, size)
    unit_key = key_wide * lax.rsqrt(jnp.sum(key_wide * key_wide, axis=-1, keepdims=True) + epsilon)
    matrix = memory.reshape(count, heads, size, size)
    recall = jnp.einsum("bhk,bhkv->bhv", unit_key, matrix, precision=highest)
    retain = jnp.exp(log_decay)[:, :, None, None]
    scaled = strength[:, :, None]
    erased = matrix - jnp.einsum("bhk,bhv->bhkv", unit_key, scaled * recall, precision=highest)
    written = jnp.einsum("bhk,bhv->bhkv", unit_key, scaled * value_wide, precision=highest)
    updated = retain * erased + written
    readout = jnp.einsum("bhk,bhkv->bhv", query_wide, updated, precision=highest)
    normed = readout * lax.rsqrt(jnp.mean(readout * readout, axis=-1, keepdims=True) + epsilon)
    normed = normed * head_gain * jax.nn.silu(gate_wide)
    return (
        updated.reshape(count, heads, size * size),
        normed.reshape(count, heads * size).astype(jnp.bfloat16),
    )


def plain_device(
    chips,
    tokens,
    memory,
    mix_gain,
    w_query,
    w_key,
    w_value,
    w_gate,
    w_beta,
    w_decay,
    decay_rate,
    decay_bias,
    head_gain,
    w_out,
    ffn_gain,
    w_up,
    w_down,
):
    rows = tokens.shape[0]
    owned = memory.shape[0]
    width = mix_gain.shape[0]
    chip = lax.axis_index("kv")
    core = lax.axis_index("tp")
    own_start = lax.axis_index(axes) * owned
    wide = tokens.astype(jnp.float32)

    def lifted_of(whole, gain):
        whole_wide = whole.astype(jnp.float32)
        scale = lax.rsqrt(jnp.sum(whole_wide * whole_wide, axis=1) / width + epsilon)
        return (whole_wide * gain).astype(jnp.bfloat16), scale[:, None]

    def project(value, weight):
        return jnp.dot(value, weight, preferred_element_type=jnp.float32)

    lifted_in, scale_in = lifted_of(gather_features(tokens, chips, chip, core), mix_gain)
    sent = jnp.stack(
        [
            (project(lifted_in, weight) * scale_in).astype(jnp.bfloat16)
            for weight in (w_query, w_key, w_value, w_gate)
        ],
        axis=1,
    )
    strength_all = jax.nn.sigmoid(project(lifted_in, w_beta) * scale_in)
    decay_all = -decay_rate * jax.nn.softplus(project(lifted_in, w_decay) * scale_in + decay_bias)
    strength = lax.dynamic_slice_in_dim(strength_all, own_start, owned, 0)
    log_decay = lax.dynamic_slice_in_dim(decay_all, own_start, owned, 0)

    part = sent.shape[2]
    leaving = by_distance(sent.reshape(chips, 2, owned, 4, part), chip)
    mine = jnp.stack(far([leaving[d] for d in range(chips)], chips))
    other = near(mine)
    pick = lambda both: jnp.where(core == 0, both[:, 0], both[:, 1])
    whole = merge(pick(mine), pick(other), chip, core)
    whole = jnp.transpose(whole, (2, 1, 0, 3)).reshape(4, owned, 2 * chips * part)
    updated, mixed = delta_step(
        whole[0], whole[1], whole[2], whole[3], strength, log_decay, memory, head_gain
    )

    mixed_all = gather(mixed, chips, chip, core).reshape(rows, mixed.shape[1])
    middle = (wide + project(mixed_all, w_out)).astype(jnp.bfloat16)
    middle_wide = middle.astype(jnp.float32)
    lifted_mid, scale_mid = lifted_of(gather_features(middle, chips, chip, core), ffn_gain)
    raised = project(lifted_mid, w_up)
    hidden = jnp.square(jax.nn.relu(raised * scale_mid)).astype(jnp.bfloat16)
    terms = project(hidden, w_down).astype(jnp.bfloat16)

    features = tokens.shape[1]
    blocks = jnp.stack([terms[:, i * 2 * features : (i + 1) * 2 * features] for i in range(chips)])
    leaving = by_distance(blocks, chip)
    total = sum(
        (got.astype(jnp.float32) for got in far([leaving[d] for d in range(chips)], chips))
    )
    low, high = total[:, :features], total[:, features:]
    arrived = near(jnp.where(core == 0, high, low))
    down = jnp.where(core == 0, low, high) + arrived
    layer_out = (middle_wide + down).astype(jnp.bfloat16)
    return (layer_out, updated)


def place():
    return lax.axis_index("kv"), lax.axis_index("tp")


def mine_lane(d):
    chip, core = place()
    return 2 * (chip ^ d) + (core if d == 0 else 1 - core)


def other_lane(d):
    chip, core = place()
    return 2 * (chip ^ d) + (1 - core if d == 0 else core)


def span(lane, size):
    return pl.ds(pl.multiple_of(lane * size, size), size)


def dot_rows(left, right):
    return lax.dot_general(left, right, (((1,), (1,)), ((), ())), preferred_element_type=jnp.float32)


def dot(left, right):
    return jnp.dot(left, right, preferred_element_type=jnp.float32)


def call(body, outs, args, scratch=(), work=1e9):
    vmem = pl.BlockSpec(memory_space=pltpu.VMEM)
    return pl.pallas_call(
        body,
        out_shape=[jax.ShapeDtypeStruct(shape, kind) for shape, kind in outs],
        in_specs=[vmem] * len(args),
        out_specs=[vmem] * len(outs),
        scratch_shapes=list(scratch),
        compiler_params=pltpu.CompilerParams(vmem_limit_bytes=16 << 20),
        cost_estimate=pl.CostEstimate(flops=int(work), bytes_accessed=0, transcendentals=0),
    )(*args)


def keep_near(tokens, near_ref):
    near_ref[...] = tokens[...]


def project_piece(piece, lane, gain, weights, lifted, parts):
    size = piece.shape[1]
    wide = piece.astype(jnp.float32)
    ready = (wide * gain[:, span(lane, size)]).astype(jnp.bfloat16)
    lifted[:, span(lane, size)] = ready
    stacked = jnp.concatenate([weight[:, span(lane, size)] for weight in weights], axis=0)
    parts.append((dot_rows(ready, stacked), jnp.sum(wide * wide, axis=1, keepdims=True)))


def project_first(chips, tokens, partner, *refs):
    got, (gain, *rest) = refs[: chips - 1], refs[chips - 1 :]
    weights, (total, squares, lifted) = rest[:4], rest[4:]
    lifted[...] = jnp.zeros_like(lifted)
    parts = []
    project_piece(tokens[...], mine_lane(0), gain, weights, lifted, parts)
    project_piece(partner[...], other_lane(0), gain, weights, lifted, parts)
    for d in range(1, chips):
        project_piece(got[d - 1][...], mine_lane(d), gain, weights, lifted, parts)
    total[...] = sum(part[0] for part in parts)
    squares[...] = jnp.broadcast_to(sum(part[1] for part in parts), squares.shape)


def project_rest(chips, others, before, before_squares, before_lifted, gain, *rest):
    weights, (scale_ref, lifted, early, farthest), sent = rest[:4], rest[4:-1], rest[-1]
    lifted[...] = before_lifted[...]
    parts = [(before[...], before_squares[:, :1])]
    for d in range(1, chips):
        project_piece(others[d - 1], other_lane(d), gain, weights, lifted, parts)
    squares = sum(part[1] for part in parts)
    scale = lax.rsqrt(squares / lifted.shape[1] + epsilon)
    total = sum(part[0] for part in parts) * scale
    sent[...] = total.astype(jnp.bfloat16).astype(jnp.float32)
    scale_ref[...] = jnp.broadcast_to(scale, scale_ref.shape)
    chip, _ = place()
    for d in range(chips):
        for c in range(2):
            row = sent[pl.ds(2 * (chip ^ d) + c, 1), :]
            if d < chips - 1:
                early[d, c : c + 1, :] = row
            else:
                farthest[c : c + 1, :] = row


def column(row, heads):
    there = lax.broadcasted_iota(jnp.int32, (heads, heads), 0)
    here = lax.broadcasted_iota(jnp.int32, (heads, heads), 1)
    return jnp.sum(jnp.where(there == here, row, 0.0), axis=1, keepdims=True)


def gates(lifted, scale, w_beta, w_decay, rate, bias, *outs):
    heads = w_beta.shape[0]
    beta_all, decay_all = dot_rows(w_beta[...], lifted[...]), dot_rows(w_decay[...], lifted[...])
    bias_column, rate_column = column(bias[...], heads), column(rate[...], heads)
    for lane, (strength, retain) in ((mine_lane(0), outs[:2]), (other_lane(0), outs[2:])):
        scale_own = scale[pl.ds(lane, 1), :][:, :1]
        here = lax.broadcasted_iota(jnp.int32, beta_all.shape, 1) == lane

        def own(every):
            return jnp.sum(jnp.where(here, every, 0.0), axis=1, keepdims=True) * scale_own

        value = own(decay_all) + bias_column
        soft = jnp.maximum(value, 0.0) + jnp.log1p(jnp.exp(-jnp.abs(value)))
        decay = jnp.exp(-rate_column * soft)
        beta = 1.0 / (1.0 + jnp.exp(-own(beta_all)))
        strength[...] = jnp.broadcast_to(beta, strength.shape)
        retain[...] = jnp.broadcast_to(decay, retain.shape)


def read_row(chips, row, mine, other, strength, retain, terms, head_gain, parts):
    heads, size = strength.shape
    chip, core = place()
    part = mine.shape[2] // 4
    across = 2 * part // size
    for there in range(chips):
        d = chip ^ there
        own = mine[d, pl.ds(row, 1), :]
        partner = other[d, pl.ds(row, 1), :]
        straight = (d == 0) == (core == 0)
        low = jnp.where(straight, own, partner)
        high = jnp.where(straight, partner, own)
        for t in range(4):
            cut = slice(t * part, (t + 1) * part)
            pair = jnp.concatenate([low[:, cut], high[:, cut]], axis=1)
            for i in range(across):
                h = there * across + i
                parts[t, h : h + 1, :] = pair[:, i * size : (i + 1) * size]
    query, key, value, gate = parts[0], parts[1], parts[2], parts[3]
    shrink = lax.rsqrt(jnp.sum(key * key, axis=1, keepdims=True) + epsilon)
    pair_of = lambda h: terms[h] if terms.dtype == jnp.bfloat16 else two_terms(terms[h])
    padded = -(-heads // 16) * 16
    pad = [jnp.zeros((padded - heads, size), jnp.float32)] if padded > heads else []
    left = jnp.concatenate([key, *pad, query, *pad], axis=0).astype(jnp.bfloat16)
    at = lax.rem(lax.broadcasted_iota(jnp.int32, (2 * padded, 2 * size), 0), padded)
    found = sum(jnp.where(at == h, dot(left, pair_of(h)), 0.0) for h in range(heads))
    found = found[:, :size] + found[:, size:]
    recall, read = found[:heads] * shrink, found[padded : padded + heads]
    write = shrink * strength[...] * (value - retain[...] * recall)
    readout = retain[...] * read + jnp.sum(key * query, axis=1, keepdims=True) * write
    normed = readout * lax.rsqrt(jnp.mean(readout * readout, axis=1, keepdims=True) + epsilon)
    normed = normed * head_gain[...] * (gate / (1.0 + jnp.exp(-gate)))
    return normed.astype(jnp.bfloat16).astype(jnp.float32), key, write


def read_memory(chips, mine, other, *refs):
    outer, (head_gain, mixed, key_ref, write_ref, parts) = refs[:6], refs[6:]
    heads, size = key_ref.shape
    _, core = place()
    given = ((core, outer[0:3]), (1 - core, outer[3:6]))
    rows = [
        read_row(chips, row, mine, other, *three, head_gain, parts.at[i])
        for i, (row, three) in enumerate(given)
    ]
    own, partner = rows[0][0], rows[1][0]
    ordered = jnp.where(core == 0, own, partner), jnp.where(core == 0, partner, own)
    for h in range(heads):
        for c in range(2):
            mixed[c : c + 1, h * size : (h + 1) * size] = ordered[c][h : h + 1]
    key_ref[...] = rows[0][1]
    write_ref[...] = rows[0][2]


def two_terms(matrix):
    high = matrix.astype(jnp.bfloat16)
    low = (matrix - high.astype(jnp.float32)).astype(jnp.bfloat16)
    return jnp.concatenate([high, low], axis=1)


def split_memory(memory, terms):
    size = memory.shape[2]
    for h in range(memory.shape[0]):
        left = memory[h]
        for i in range(2):
            term = left.astype(jnp.bfloat16)
            terms[h, :, i * size : (i + 1) * size] = term
            left = left - term.astype(jnp.float32)


def update_memory(memory, key, write, retain, updated):
    heads, size = key.shape
    rest = jnp.zeros((size - heads, size), jnp.float32)
    turned = jnp.concatenate([key[...], rest], axis=0).T
    for h in range(heads):
        row = slice(h, h + 1)
        updated[h] = retain[row, :] * memory[h] + turned[:, row] * write[row, :]


def by_core(own, partner):
    first = place()[1] == 0
    low, high = jnp.where(first, own, partner), jnp.where(first, partner, own)
    return jnp.concatenate([low, high], axis=-1)


def chip_at(distance):
    chip, core = place()
    return chip ^ jnp.where(core == 0, distance[0], distance[1])


def mix_out(distances, tokens, partner_tokens, *refs):
    count = len(distances)
    got, (weight, partner_weight, block, middle, rows, wide) = refs[:count], refs[count:]
    for piece, distance in zip(got, distances):
        for c in range(2):
            rows[pl.ds(2 * chip_at(distance) + c, 1), :] = piece[c : c + 1, :]
    left = rows[...].astype(jnp.bfloat16)
    branch = by_core(dot(left, weight[...]), dot(left, partner_weight[...]))
    whole = branch + by_core(tokens[...].astype(jnp.float32), partner_tokens[...].astype(jnp.float32))
    block[...] = whole.astype(jnp.bfloat16)
    wide[...] = whole
    middle[...] = wide[:, span(place()[1], middle.shape[1])].astype(jnp.bfloat16)


def up_pieces(got, distances, gain, weight, parts):
    for piece, distance in zip(got, distances):
        size, there = piece.shape[1], chip_at(distance)
        wide = piece[...].astype(jnp.float32)
        ready = (wide * gain[:, span(there, size)]).astype(jnp.bfloat16)
        squares = jnp.sum(wide * wide, axis=1, keepdims=True)
        parts.append((dot(ready, weight[span(there, size), :]), squares))


def up_first(distances, *refs):
    count = len(distances)
    got, (gain, weight, total, squares) = refs[:count], refs[count:]
    parts = []
    up_pieces(got, distances, gain, weight, parts)
    total[...] = sum(part[0] for part in parts)
    squares[...] = jnp.broadcast_to(sum(part[1] for part in parts), squares.shape)


def up_rest(chips, distances, *refs):
    count = len(distances)
    got, rest = refs[:count], refs[count:]
    *before, gain, weight, down, hidden_ref, leaving, farthest = rest
    parts = [(a[...], b[:, :1]) for a, b in zip(before[::2], before[1::2])]
    up_pieces(got, distances, gain, weight, parts)
    scale = lax.rsqrt(sum(part[1] for part in parts) / gain.shape[1] + epsilon)
    raised = jnp.maximum(sum(part[0] for part in parts) * scale, 0.0)
    hidden = (raised * raised).astype(jnp.bfloat16)
    hidden_ref[...] = hidden
    size = leaving.shape[2]
    for d in range(chips - 1):
        leaving[d] = dot(hidden, down[:, span(other_lane(d), size)]).astype(jnp.bfloat16)
    across = span(place()[0] ^ (chips - 1), 2 * size)
    farthest[...] = dot(hidden, down[:, across]).astype(jnp.bfloat16)


def down_own(d, hidden, down, arrived, total):
    own = dot(hidden[...], down[:, span(mine_lane(d), total.shape[1])])
    total[...] = (own + arrived[d].astype(jnp.float32)).astype(total.dtype)


def add_up(middle, own, farthest, passed, *refs):
    *got, out = refs
    half = span(place()[1], out.shape[1])
    total = own[...]
    for piece in (farthest[:, half], passed[:, half], *(piece[...] for piece in got)):
        total = total + piece.astype(jnp.float32)
    out[...] = (middle[...].astype(jnp.float32) + total).astype(jnp.bfloat16)


def kernel_device(
    chips,
    tokens,
    memory,
    mix_gain,
    w_query,
    w_key,
    w_value,
    w_gate,
    w_beta,
    w_decay,
    decay_rate,
    decay_bias,
    head_gain,
    w_out,
    ffn_gain,
    w_up,
    w_down,
):
    f32, bf16 = jnp.float32, jnp.bfloat16
    rows, features = tokens.shape
    width = mix_gain.shape[0]
    heads = w_beta.shape[1]
    size = head_gain.shape[0]
    units = w_up.shape[1]
    part = w_query.shape[1]

    got = far([tokens] * chips, chips)[1:]
    partner = near(tokens)
    (tokens,) = call(keep_near, [(tokens.shape, bf16)], [tokens], work=8e9)
    others = near(jnp.stack(got))
    weights = [weight.T for weight in (w_query, w_key, w_value, w_gate)]
    gain_in = mix_gain.reshape(1, width)
    total, squares, lifted = call(
        functools.partial(project_first, chips),
        [((rows, 4 * part), f32), ((rows, 128), f32), ((rows, width), bf16)],
        [tokens, partner, *got, gain_in, *weights],
    )
    scale_in, lifted, early, farthest = call(
        functools.partial(project_rest, chips),
        [((rows, 128), f32), ((rows, width), bf16)]
        + [((chips - 1, 2, 4 * part), f32), ((2, 4 * part), f32)],
        [others, total, squares, lifted, gain_in, *weights],
        [pltpu.VMEM((rows, 4 * part), f32)],
    )
    strength, retain, partner_strength, partner_retain = call(
        gates,
        [((heads, size), f32)] * 4,
        [lifted, scale_in, w_beta.T, w_decay.T]
        + [value.reshape(1, heads) for value in (decay_rate, decay_bias)],
    )
    passed = near(early)
    both = [jnp.stack([early[d], passed[d]]) for d in range(chips - 1)]
    got = far(both + [farthest], chips)
    mine = jnp.stack([piece[0] for piece in got[:-1]] + [got[-1]])
    other = jnp.stack([piece[1] for piece in got[:-1]] + [near(got[-1])])
    matrix = memory.reshape(heads, size, size)
    shape = ((heads, size, 2 * size), bf16)
    (terms,) = call(split_memory, [shape], [matrix], work=5e8)
    moved = near(matrix)
    mixed, key, write = call(
        functools.partial(read_memory, chips),
        [((2, heads * size), f32), ((heads, size), f32), ((heads, size), f32)],
        [mine, other, strength, retain, terms, partner_strength, partner_retain, moved]
        + [head_gain.reshape(1, size)],
        [pltpu.VMEM((2, 4, heads, size), f32)],
    )
    (updated,) = call(
        update_memory, [((heads, size, size), f32)], [matrix, key, write, retain], work=5e8
    )

    here = (0, 0)
    direct, passed = shared(mixed, chips)
    got, distances = zip((mixed, here), *direct, *passed)
    block, middle = call(
        functools.partial(mix_out, distances),
        [((rows, 2 * features), bf16), ((rows, features), bf16)],
        [tokens, partner, *got, w_out, near(w_out)],
        [pltpu.VMEM((rows, heads * size), f32), pltpu.VMEM((rows, 2 * features), f32)],
    )

    direct, passed = shared(block, chips)
    gain_mid = ffn_gain.reshape(1, width)
    sums = [((rows, units), f32), ((rows, 128), f32)]
    early = []
    for piece, distance in [(block, here), *direct[:-1]]:
        early += call(functools.partial(up_first, [distance]), sums, [piece, gain_mid, w_up])
    got, distances = zip(direct[-1], *passed)
    hidden, leaving, farthest = call(
        functools.partial(up_rest, chips, distances),
        [((rows, units), bf16), ((chips - 1, rows, features), bf16), ((rows, 2 * features), bf16)],
        [*got, *early, gain_mid, w_up, w_down],
    )
    arrived = near(leaving)
    terms = []
    for d in range(chips - 1):
        terms += call(
            functools.partial(down_own, d),
            [((rows, features), bf16 if d else f32)],
            [hidden, w_down, arrived],
        )
    own = terms[0]
    terms.append(farthest)
    *got, farthest = far(terms, chips)[1:]
    (layer_out,) = call(
        add_up,
        [((rows, features), bf16)],
        [middle, own, farthest, near(farthest), *got],
    )
    return (layer_out, updated.reshape(memory.shape))


def per_device(chips, *arrays):
    tokens, memory, head_gain = arrays[0], arrays[1], arrays[11]
    fits = (
        memory.shape[0] == 1
        and tokens.shape[0] == 2 * chips
        and tokens.shape[1] % 128 == 0
        and arrays[3].shape[1] % 16 == 0
        and 2 * arrays[3].shape[1] % head_gain.shape[0] == 0
        and head_gain.shape[0] == 128
        and memory.shape[1] <= 128
    )
    return (kernel_device if fits else plain_device)(chips, *arrays)


def solution(mesh):
    chips = mesh.shape["kv"]
    placed = (
        P(("grp", "dp"), ("kv", "tp")),
        P(("grp", "dp", "kv", "tp"), None, None),
        P(),
        P(None, ("kv", "tp")),
        P(None, ("kv", "tp")),
        P(None, ("kv", "tp")),
        P(None, ("kv", "tp")),
        P(),
        P(),
        P(),
        P(),
        P(),
        P(None, ("kv", "tp")),
        P(),
        P(None, ("kv", "tp")),
        P(("kv", "tp"), None),
    )

    def step(*arrays):
        return per_device(chips, *arrays)

    return jax.shard_map(
        step,
        mesh=mesh,
        in_specs=placed,
        out_specs=(P(("grp", "dp"), ("kv", "tp")), P(("grp", "dp", "kv", "tp"), None, None)),
        check_vma=False,
    )
```
